128 devices in a mesh: sp: 16 (over z, y), tp: 8 (over x, core).
Axes of the slice: x: 4, y: 4, z: 4, core: 2. Of those that a mesh axis runs over, the one named last changes fastest.
Arguments:
- tokens: bfloat16 [12288, 2048], P('sp'), may hold values from -6 to 6
- norm_gain: float32 [2048], replicated, may hold values from 0.5 to 80
- grid_query_weight: bfloat16 [2048, 2048], P(None, 'tp'), may hold values from -0.5 to 0.5
- grid_key_weight: bfloat16 [2048, 1024], P(None, 'tp'), may hold values from -0.5 to 0.5
- grid_value_weight: bfloat16 [2048, 1024], P(None, 'tp'), may hold values from -0.5 to 0.5
- grid_query_gain: float32 [128], replicated, may hold values from 1.6 to 6
- grid_key_gain: float32 [128], replicated, may hold values from 1.6 to 6
- local_query_weight: bfloat16 [2048, 2048], P(None, 'tp'), may hold values from -0.5 to 0.5
- local_key_weight: bfloat16 [2048, 1024], P(None, 'tp'), may hold values from -0.5 to 0.5
- local_value_weight: bfloat16 [2048, 1024], P(None, 'tp'), may hold values from -0.5 to 0.5
- sink_logit: float32 [16], P('tp'), may hold values from 1 to 6
- grid_out_weight: bfloat16 [2048, 2048], P('tp'), may hold values from -0.09375 to 0.09375
- local_out_weight: bfloat16 [2048, 2048], P('tp'), may hold values from -0.09375 to 0.09375
Outputs:
- mixed: bfloat16 [12288, 2048], P(('sp', 'tp'))
The draws below stay inside these ranges and needn't reach their ends.
All inputs are finite; a program needn't handle non-finite values.
Results may differ from the reference program's by a relative error of at most 0.03.
Values may be sent and summed in bfloat16 or wider, within the bound.
A program may use at most 192 MiB of HBM per device.

```python
import jax
import jax.numpy as jnp
from jax import lax

D = 2048
HEAD = 128
GRID_HEADS = 16
GRID_KV = 8
LOCAL_HEADS = 16
LOCAL_KV = 8
WINDOW = 128
GRID_W = 64
SEQ = 12288
N_TP = 8


def shared_weight(key, salt, heads):
    drawn = jax.random.normal(jax.random.fold_in(key, salt), (D, heads * HEAD), jnp.float32) * D ** (-0.5)
    return jnp.clip(drawn, -0.5, 0.5)


def paired_key(key, salt, heads, groups):
    return shared_weight(key, salt + 1, groups)


def draw_grid_query_weight(key, part):
    return shared_weight(key, 101, GRID_HEADS).astype(jnp.bfloat16)


def draw_grid_key_weight(key, part):
    return paired_key(key, 101, GRID_HEADS, GRID_KV).astype(jnp.bfloat16)


def draw_local_query_weight(key, part):
    return shared_weight(key, 301, LOCAL_HEADS).astype(jnp.bfloat16)


def draw_local_key_weight(key, part):
    return paired_key(key, 301, LOCAL_HEADS, LOCAL_KV).astype(jnp.bfloat16)


def draw_norm_gain(key, part):
    base = jax.random.uniform(jax.random.fold_in(key, 201), (D,), jnp.float32, 0.5, 1.5)
    return base


def head_gain(key, salt):
    return jax.random.uniform(jax.random.fold_in(key, salt), (HEAD,), jnp.float32, 1.6, 2.4)


def draw_grid_query_gain(key, part):
    return head_gain(key, 401)


def draw_grid_key_gain(key, part):
    return head_gain(key, 402)


def level_of(key, dims, pieces, low, high):
    def one(dim, parts):
        draws = jax.random.uniform(jax.random.fold_in(jax.random.fold_in(key, 6), dim), (parts,), jnp.float32, low / len(pieces), high / len(pieces))
        return jnp.repeat(jnp.exp(draws), dims[dim] // parts).reshape((-1,) + (1,) * (len(dims) - dim - 1))

    level = one(*pieces[0])
    for cut in pieces[1:]:
        level = level * one(*cut)
    return level


def normal_values(key, dims, scale, reach, cuts=(), kind=jnp.bfloat16):
    entries = scale * jax.random.normal(key, dims, jnp.float32)
    if cuts:
        entries = entries * level_of(key, dims, cuts, -0.22, 0.18)
    return jnp.clip(entries, -reach, reach).astype(kind)


def setup_inputs(seed: int = 0) -> dict:
    key_list = jax.random.split(jax.random.key(seed), 14)
    return {
        "tokens": normal_values(key_list[0], (SEQ, D), 1.0, 6.0, ((0, 16),)),
        "norm_gain": draw_norm_gain(jax.random.fold_in(key_list[13], 71), 0),
        "grid_query_weight": draw_grid_query_weight(jax.random.fold_in(key_list[13], 71), 0),
        "grid_key_weight": draw_grid_key_weight(jax.random.fold_in(key_list[13], 71), 0),
        "grid_value_weight": normal_values(key_list[4], (D, GRID_KV * HEAD), (D // 16) ** -0.5, 0.5, ((1, 8),)),
        "grid_query_gain": draw_grid_query_gain(jax.random.fold_in(key_list[13], 71), 0),
        "grid_key_gain": draw_grid_key_gain(jax.random.fold_in(key_list[13], 71), 0),
        "local_query_weight": draw_local_query_weight(jax.random.fold_in(key_list[13], 71), 0),
        "local_key_weight": draw_local_key_weight(jax.random.fold_in(key_list[13], 71), 0),
        "local_value_weight": normal_values(key_list[9], (D, LOCAL_KV * HEAD), (D // 16) ** -0.5, 0.5, ((1, 8),)),
        "sink_logit": jnp.clip(1.0 + 5.0 * jax.random.uniform(key_list[10], (LOCAL_HEADS,), jnp.float32) ** level_of(key_list[10], (LOCAL_HEADS,), ((0, 8),), -0.2, 0.2), 1.0, 6.0),
        "grid_out_weight": normal_values(key_list[11], (GRID_HEADS * HEAD, D), (GRID_HEADS * HEAD + LOCAL_HEADS * HEAD) ** -0.5, 0.09375, ((0, 8),)),
        "local_out_weight": normal_values(key_list[12], (LOCAL_HEADS * HEAD, D), (GRID_HEADS * HEAD + LOCAL_HEADS * HEAD) ** -0.5, 0.09375, ((0, 8),)),
    }


EPSILON = 1e-06
ROPE_BASE = 10000.0

def rms_rows(values, gain):
    widened = values.astype(jnp.float32)
    return widened * lax.rsqrt(lax.optimization_barrier(jnp.mean(widened * widened, axis=-1, keepdims=True)) + EPSILON) * gain

def half_turn(part, angles):
    cosine = jnp.cos(angles)
    sine = jnp.sin(angles)
    cosine = jnp.concatenate([cosine, cosine], axis=-1)
    sine = jnp.concatenate([sine, sine], axis=-1)
    first, second = jnp.split(part, 2, axis=-1)
    turned = jnp.concatenate([-second, first], axis=-1)
    return part * cosine + turned * sine

def axial_turn(heads, positions):
    half_dim = heads.shape[-1] // 2
    inverse = ROPE_BASE ** (-jnp.arange(0, half_dim, 2, dtype=jnp.float32) / half_dim)
    row_angle = (positions // GRID_W).astype(jnp.float32)[:, None, None] * inverse
    col_angle = (positions % GRID_W).astype(jnp.float32)[:, None, None] * inverse
    return jnp.concatenate([half_turn(heads[..., :half_dim], row_angle), half_turn(heads[..., half_dim:], col_angle)], axis=-1)

def rounded_part(outs, weight, index, width):
    picked = lax.dynamic_slice_in_dim(outs, (index * width).astype(jnp.int32), width, 1)
    rows = lax.dynamic_slice_in_dim(weight, (index * width).astype(jnp.int32), width, 0)
    product = jnp.dot(picked, rows, preferred_element_type=jnp.float32).astype(jnp.bfloat16)
    return lax.optimization_barrier(product).astype(jnp.float32)

def reference(tokens, norm_gain, grid_query_weight, grid_key_weight, grid_value_weight, grid_query_gain, grid_key_gain, local_query_weight, local_key_weight, local_value_weight, sink_logit, grid_out_weight, local_out_weight):
    seq_len = tokens.shape[0]
    positions = jnp.arange(seq_len, dtype=jnp.int32)
    normed = rms_rows(tokens, norm_gain).astype(jnp.bfloat16)

    def project(weight):
        return jnp.dot(normed, weight, preferred_element_type=jnp.float32).astype(jnp.bfloat16)
    group_size = GRID_HEADS // GRID_KV
    score_scale = HEAD ** (-0.5)
    queries = axial_turn(rms_rows(project(grid_query_weight).reshape(seq_len, GRID_HEADS, HEAD), grid_query_gain), positions).astype(jnp.bfloat16).reshape(seq_len, GRID_KV, group_size, HEAD)
    keys = axial_turn(rms_rows(project(grid_key_weight).reshape(seq_len, GRID_KV, HEAD), grid_key_gain), positions).astype(jnp.bfloat16)
    values = project(grid_value_weight).reshape(seq_len, GRID_KV, HEAD)
    keys_wide = keys.astype(jnp.float32)
    values_wide = values.astype(jnp.float32)
    block_rows = min(512, seq_len)

    def one_block(start):
        block_q = lax.dynamic_slice_in_dim(queries, start, block_rows, 0).astype(jnp.float32)
        scores = jnp.einsum('qhgd,shd->hgqs', block_q, keys_wide) * score_scale
        weights = jax.nn.softmax(scores, axis=-1).astype(jnp.bfloat16)
        result = jnp.einsum('hgqs,shd->qhgd', weights.astype(jnp.float32), values_wide)
        return result.astype(jnp.bfloat16)
    starts = (jnp.arange(seq_len // block_rows) * block_rows).astype(jnp.int32)
    grid_out = lax.map(one_block, starts).reshape(seq_len, GRID_HEADS * HEAD)
    local_size = LOCAL_HEADS // LOCAL_KV
    blocks = seq_len // WINDOW
    local_q = project(local_query_weight).reshape(blocks, WINDOW, LOCAL_KV, local_size, HEAD)
    local_k = project(local_key_weight).reshape(seq_len, LOCAL_KV, HEAD)
    local_v = project(local_value_weight).reshape(seq_len, LOCAL_KV, HEAD)

    def banded(values_in):
        padded = jnp.pad(values_in, ((WINDOW, WINDOW), (0, 0), (0, 0))).reshape(blocks + 2, WINDOW, LOCAL_KV, HEAD)
        return jnp.concatenate([padded[:-2], padded[1:-1], padded[2:]], axis=1)
    band_k = banded(local_k).astype(jnp.float32)
    band_v = banded(local_v).astype(jnp.float32)
    scores = jnp.einsum('nqhgd,nshd->hgnqs', local_q.astype(jnp.float32), band_k) * score_scale
    relative = jnp.arange(3 * WINDOW)[None, :] - WINDOW - jnp.arange(WINDOW)[:, None]
    key_pos = jnp.arange(blocks)[:, None] * WINDOW - WINDOW + jnp.arange(3 * WINDOW)[None, :]
    valid = (jnp.abs(relative) <= WINDOW)[None] & ((key_pos >= 0) & (key_pos < seq_len))[:, None, :]
    scores = jnp.where(valid, scores, -jnp.inf)
    sink = sink_logit.reshape(LOCAL_KV, local_size, 1, 1, 1)
    top = jnp.maximum(lax.optimization_barrier(jnp.max(scores, axis=-1, keepdims=True)), sink)
    lifted = jnp.exp(scores - top)
    weights = (lifted / (lax.optimization_barrier(jnp.sum(lifted, axis=-1, keepdims=True)) + jnp.exp(sink - top))).astype(jnp.bfloat16)
    local_out = jnp.einsum('hgnqs,nshd->nqhgd', weights.astype(jnp.float32), band_v)
    local_out = local_out.astype(jnp.bfloat16).reshape(seq_len, LOCAL_HEADS * HEAD)
    grid_width = GRID_HEADS * HEAD // N_TP
    local_width = LOCAL_HEADS * HEAD // N_TP

    def add_group(index, total):
        total = total + rounded_part(grid_out, grid_out_weight, index, grid_width)
        return total + rounded_part(local_out, local_out_weight, index, local_width)
    total = lax.fori_loop(0, N_TP, add_group, jnp.zeros((seq_len, D), jnp.float32))
    return total.astype(jnp.bfloat16)
```

```python
import functools
import math

import jax
import jax.numpy as jnp
import numpy as np
from jax import lax
from jax.experimental import pallas as pl
from jax.experimental.pallas import tpu as pltpu
from jax.sharding import PartitionSpec as P

D = 2048
HEAD = 128
WINDOW = 128
GRID_W = 64
ROWS = 768
EPSILON = 1e-06
ROPE_BASE = 10000.0
LOG2E = math.log2(math.e)
SCORE = HEAD ** (-0.5) * LOG2E
NSP = 16
SIDE = 4
BLOCKS = 4
PART = 48
TILES = 5
EARLY = 40
BF = jnp.bfloat16
F32 = jnp.float32
MESH = pl.DeviceIdType.MESH


def dot(a, b):
    return jnp.dot(a, b, preferred_element_type=F32)


def rope_tables():
    half = HEAD // 2
    inverse = ROPE_BASE ** (-np.arange(0, half, 2, dtype=np.float64) / half)
    sign = np.concatenate([-np.ones(half // 2), np.ones(half // 2)])

    def table(count):
        angle = np.arange(count)[:, None] * np.concatenate([inverse, inverse])
        return np.cos(angle), np.sin(angle) * sign

    rows = np.zeros((2, NSP, 16, HEAD), np.float32)
    cosine, sine = table(NSP * ROWS // GRID_W)
    per = ROWS // GRID_W
    rows[0, :, :per, :half] = cosine.reshape(NSP, per, half)
    rows[1, :, :per, :half] = sine.reshape(NSP, per, half)
    cols = np.zeros((2, GRID_W, HEAD), np.float32)
    cosine, sine = table(GRID_W)
    cols[0, :, half:] = cosine
    cols[1, :, half:] = sine
    return np.ascontiguousarray(rows.transpose(1, 0, 2, 3)), cols


def kernel(
    tokens,
    gain,
    wq,
    wk,
    wv,
    gain_q,
    gain_k,
    lwq,
    lwk,
    lwv,
    sink,
    wog,
    wol,
    row_table,
    col_table,
    out,
    xs,
    xn,
    wg,
    wl,
    wo,
    rows_tab,
    qr,
    qs,
    qp,
    kall,
    vall,
    m,
    l,
    o,
    s0,
    s1,
    lq,
    lk,
    lv,
    lo,
    osend,
    orecv,
    keep,
    dsend,
    drecv,
    x0,
    x12,
    ra,
    r1,
    in_sem,
    kv_s,
    kv_r,
    q_s,
    q_r,
    h_s,
    h_r,
    o_s,
    o_r,
    d_s,
    d_r,
    x_s,
    x_r,
):
    sp = lax.axis_index("sp")
    tp = lax.axis_index("tp")
    core = lax.rem(tp, 2)
    x = tp // 2
    z = sp // SIDE
    y = lax.rem(sp, SIDE)

    def along_z(d):
        return lax.rem(z + d, SIDE) * SIDE + y

    def along_y(d):
        return z * SIDE + lax.rem(y + d, SIDE)

    def q_peer(d):
        return {"sp": along_z(d) * (1 - core) + along_y(d) * core, "tp": tp}

    def kv_peer(d):
        return {"sp": along_z(d) * core + along_y(d) * (1 - core), "tp": tp}

    def sp_peer(d):
        return {"sp": lax.rem(sp + d, NSP), "tp": tp}

    def x_peer(d):
        return {"sp": sp, "tp": lax.rem(x + d, SIDE) * 2 + core}

    partner = {"sp": sp, "tp": x * 2 + 1 - core}

    def remote(src, dst, send, recv, peer):
        return pltpu.make_async_remote_copy(
            src_ref=src, dst_ref=dst, send_sem=send, recv_sem=recv, device_id=peer, device_id_type=MESH
        )

    def local(src, dst, i):
        return pltpu.make_async_copy(src, dst, in_sem.at[i])

    third = ROWS // 3
    loads = [
        local(tokens.at[pl.ds(0, third)], xs.at[pl.ds(0, third)], 0),
        local(wk, wg.at[:, pl.ds(256, 128)], 1),
        local(wv, wg.at[:, pl.ds(384, 128)], 2),
        local(wq, wg.at[:, pl.ds(0, 256)], 3),
        local(row_table.at[sp], rows_tab, 4),
        local(tokens.at[pl.ds(third, third)], xs.at[pl.ds(third, third)], 5),
        local(tokens.at[pl.ds(2 * third, third)], xs.at[pl.ds(2 * third, third)], 6),
        local(lwq, wl.at[:, pl.ds(0, 256)], 7),
        local(lwk, wl.at[:, pl.ds(256, 128)], 8),
        local(lwv, wl.at[:, pl.ds(384, 128)], 9),
        local(wog, wo.at[pl.ds(0, 256)], 10),
        local(wol, wo.at[pl.ds(256, 256)], 11),
    ]
    for load in loads:
        load.start()

    barrier = pltpu.get_barrier_semaphore()
    peers = [q_peer(1), q_peer(2), q_peer(3), kv_peer(1), kv_peer(3), sp_peer(1), sp_peer(NSP - 1)]
    peers += [x_peer(1), x_peer(3), partner]
    for peer in peers:
        pl.semaphore_signal(barrier, inc=1, device_id=peer, device_id_type=MESH)

    m[...] = jnp.full_like(m, -1e30)
    l[...] = jnp.zeros_like(l)
    o[...] = jnp.zeros_like(o)
    vall[:, pl.ds(HEAD, 16), :] = jnp.ones((SIDE, 16, ROWS), BF)

    lane = lax.broadcasted_iota(jnp.int32, (third, HEAD), 1)
    first_half = lax.rem(lane, 64) < 32

    def norm(r):
        block = xs[pl.ds(r * third, third), :].astype(F32)
        mean = jnp.mean(block * block, axis=-1, keepdims=True)
        xn[pl.ds(r * third, third), :] = (block * lax.rsqrt(mean + EPSILON) * gain[...]).astype(BF)

    def rope(u, gain_row, r):
        mean = jnp.mean(u * u, axis=-1, keepdims=True)
        u = u * lax.rsqrt(mean + EPSILON) * gain_row
        swapped = jnp.where(first_half, pltpu.roll(u, HEAD - 32, 1), pltpu.roll(u, 32, 1))
        per = third // GRID_W

        def table(which):
            return jnp.concatenate(
                [col_table[which] + rows_tab[which, pl.ds(r * per + i, 1), :] for i in range(per)], axis=0
            )

        return (u * table(0) + swapped * table(1)).astype(BF)

    def project_grid(r):
        rows = pl.ds(r * third, third)
        p = dot(xn[rows, :], wg[...])
        kall[0, rows, :] = rope(p[:, 256:384], gain_k[...], r)
        vall[0, pl.ds(0, HEAD), rows] = p[:, 384:512].T.astype(BF)
        scaled = gain_q[...] * SCORE
        qr[0, rows, :] = rope(p[:, 0:128], scaled, r)
        qr[1, rows, :] = rope(p[:, 128:256], scaled, r)

    loads[0].wait()
    norm(0)
    for i in (1, 2, 3, 4, 5):
        loads[i].wait()
    norm(1)
    project_grid(0)
    loads[6].wait()
    norm(2)
    project_grid(1)
    project_grid(2)

    pl.semaphore_wait(barrier, len(peers))
    value_rows = pl.ds(0, HEAD)
    sends = []

    def send(*args):
        copy = remote(*args)
        copy.start()
        sends.append(copy)

    def k_copy(slot_from, slot_to, s, d):
        return (kall.at[slot_from], kall.at[slot_to], kv_s.at[s], kv_r.at[0, slot_to], kv_peer(d))

    def v_copy(slot_from, slot_to, s, d):
        return (
            vall.at[slot_from, value_rows],
            vall.at[slot_to, value_rows],
            kv_s.at[s],
            kv_r.at[1, slot_to],
            kv_peer(d),
        )

    k_up, k_down = k_copy(0, 3, 0, 1), k_copy(0, 1, 1, 3)
    v_up, v_down = v_copy(0, 3, 2, 1), v_copy(0, 1, 3, 3)
    for args in (k_up, v_down, k_down, v_up):
        send(*args)
    k_relay, v_relay = k_copy(3, 2, 4, 1), v_copy(1, 2, 5, 3)

    ahead, behind, across = (lax.rem(x + d, SIDE) * 192 for d in (1, 3, 2))
    own = x * 192
    starts = (
        (across, across + 48, across + 96, across + 144),
        (ahead, behind, ahead + 96, behind + 96),
        (ahead + 48, behind + 48, ahead + 144, behind + 144),
        (own, own + 48, own + 96, own + 144),
    )

    def gather(ref, k):
        return jnp.concatenate([ref[pl.ds(pl.multiple_of(s, 16), PART), :] for s in starts[k]], axis=0)

    for k in range(BLOCKS):
        one, two = gather(qr.at[0], k), gather(qr.at[1], k)
        pieces = (one[:128], jnp.concatenate([one[128:], two[:64]], axis=0), two[64:])
        for i, piece in enumerate(pieces):
            turned = piece.astype(F32).T.astype(BF)
            qs[k, i] = turned
            qp[k * 10 + 9 if i == 2 else EARLY + 2 * k + i] = turned

    place = {2: 0, 1: 3, 3: 6}

    def q_copy(source, k, slot, s, d):
        return (source, qp.at[pl.ds(k * 10 + place[slot], 3)], q_s.at[k, s], q_r.at[k, slot], q_peer(d))

    def send_queries(k):
        send(*q_copy(qs.at[k], k, 3, 0, 1))
        send(*q_copy(qs.at[k], k, 1, 1, 3))

    def relay_queries(k):
        arrived = 3 if k % 2 == 0 else 1
        wait_queries(k, arrived)
        send(*q_copy(qp.at[pl.ds(k * 10 + place[arrived], 3)], k, 2, 2, 4 - arrived))

    def wait_queries(k, slot):
        args = q_copy(qs.at[k], k, slot, 0, 1)
        remote(*args).wait_recv()

    for i in (7, 8, 9):
        loads[i].wait()
    for r in range(3):
        rows = pl.ds(r * third, third)
        p = dot(xn[rows, :], wl[...])
        lq[rows, :] = (p[:, 0:256] * SCORE).astype(BF)
        lk[pl.ds(WINDOW + r * third, third), :] = p[:, 256:384].astype(BF)
        lv[pl.ds(WINDOW + r * third, third), :] = p[:, 384:512].astype(BF)

    def halo(ref, i, low):
        source, target, d = (ROWS, 0, 1) if low else (WINDOW, ROWS + WINDOW, NSP - 1)
        j = 2 * i + (0 if low else 1)
        return (
            ref.at[pl.ds(source, WINDOW)],
            ref.at[pl.ds(target, WINDOW)],
            h_s.at[j],
            h_r.at[j],
            sp_peer(d),
        )

    halos = [halo(ref, i, low) for i, ref in enumerate((lk, lv)) for low in (True, False)]
    for args in halos:
        send(*args)

    def attend(base, tiles, slots, count):
        units = tiles * count // 2

        def where(u):
            halves = []
            for h in range(2):
                index = 2 * u + h
                halves.append((slots(index // tiles), base + 2 * lax.rem(index, tiles)))
            return halves

        def scores(u, ref):
            tops = []
            for h, (t, g) in enumerate(where(u)):
                queries = jnp.concatenate([qp[g], qp[g + 1]], axis=1)
                s = dot(kall[t], queries)
                ref[h] = s
                tops.append(jnp.max(s, axis=0, keepdims=True))
            return tops

        def weigh(u, ref, tops):
            for h, (t, g) in enumerate(where(u)):
                before = jnp.concatenate([m[g], m[g + 1]], axis=1)
                top = jnp.maximum(before, tops[h])
                factor = jnp.exp2(before - top)
                weights = jnp.exp2(ref[h] - top).astype(BF)
                result = dot(vall[t], weights)
                for i in range(2):
                    part = slice(i * 128, i * 128 + 128)
                    m[g + i] = top[:, part]
                    l[g + i] = l[g + i] * factor[:, part] + result[HEAD : HEAD + 1, part]
                    o[g + i] = o[g + i] * factor[:, part] + result[:HEAD, part]

        tops = scores(0, s0)

        def body(i, tops):
            u = 2 * i
            later = scores(u + 1, s1)
            weigh(u, s0, tops)
            tops = scores(jnp.minimum(u + 2, units - 1), s0)
            weigh(u + 1, s1, later)
            return tops

        lax.fori_loop(0, units // 2, body, tops)

    attend(EARLY, 4, lambda i: i * 0, 1)

    for args in halos:
        remote(*args).wait_recv()
    wide = 3 * WINDOW
    row = lax.rem(lax.broadcasted_iota(jnp.int32, (2 * WINDOW, wide), 0), WINDOW)
    col = lax.broadcasted_iota(jnp.int32, (2 * WINDOW, wide), 1)
    near = (col >= row) & (col <= row + 2 * WINDOW)
    sink_rows = jnp.concatenate(
        [jnp.full((WINDOW, 1), sink[0] * LOG2E, F32), jnp.full((WINDOW, 1), sink[1] * LOG2E, F32)], axis=0
    )
    blocks = ROWS // WINDOW

    def banded(n, carry):
        at = pl.multiple_of(n * WINDOW, WINDOW)
        rows = lq[pl.ds(at, WINDOW), :]
        queries = jnp.concatenate([rows[:, :HEAD], rows[:, HEAD:]], axis=0)
        keys = lk[pl.ds(at, wide), :]
        s = lax.dot_general(queries, keys, (((1,), (1,)), ((), ())), preferred_element_type=F32)
        block = sp * blocks + n
        low = jnp.where(block == 0, WINDOW, 0)
        high = jnp.where(block == NSP * blocks - 1, 2 * WINDOW, wide)
        s = jnp.where(near & (col >= low) & (col < high), s, -1e30)
        top = jnp.maximum(jnp.max(s, axis=1, keepdims=True), sink_rows)
        lifted = jnp.exp2(s - top)
        total = jnp.sum(lifted, axis=1, keepdims=True) + jnp.exp2(sink_rows - top)
        result = dot(lifted.astype(BF), lv[pl.ds(at, wide), :]) / total
        lo[pl.ds(at, WINDOW), :] = jnp.concatenate([result[:WINDOW], result[WINDOW:]], axis=1).astype(BF)
        return carry

    lax.fori_loop(0, blocks, banded, 0)

    remote(*k_up).wait_recv()
    send(*k_relay)
    remote(*v_down).wait_recv()
    send(*v_relay)
    for k in range(BLOCKS):
        send_queries(k)
    remote(*k_down).wait_recv()
    remote(*v_up).wait_recv()
    attend(EARLY, 4, lambda i: 1 + 2 * i, 2)
    relay_queries(0)
    remote(*k_relay).wait_recv()
    remote(*v_relay).wait_recv()
    attend(EARLY, 4, lambda i: i * 0 + 2, 1)
    relay_queries(1)

    def packed(g):
        total = l[g]
        level = m[g] + jnp.log2(total)
        high = level.astype(BF)
        rest = level - high.astype(F32)
        mid = rest.astype(BF)
        low = (rest - mid.astype(F32)).astype(BF)
        tail = jnp.concatenate([high, mid, low, jnp.zeros((13, HEAD), BF)], axis=0)
        return jnp.concatenate([(o[g] / total).astype(BF), tail], axis=0)

    def o_copy(k, s):
        return (osend.at[k, s], orecv.at[k, 4 - s], o_s.at[k, s], o_r.at[k, 4 - s], q_peer(s))

    def send_results(k):
        for s in (2, 1, 3):
            for i in range(3):
                osend[k, s, i] = packed(k * 10 + place[s] + i)
            send(*o_copy(k, s))

    def merge(k):
        for s in (1, 3, 2):
            remote(*o_copy(k, s)).wait_recv()
        merged = []
        for i in range(3):
            g = k * 10 + 9 if i == 2 else EARLY + 2 * k + i
            levels = []
            for s in (1, 2, 3):
                rows = orecv[k, s, i, pl.ds(HEAD, 16), :].astype(F32)
                levels.append(rows[0:1] + rows[1:2] + rows[2:3])
            total = l[g]
            mine = m[g] + jnp.log2(total)
            top = functools.reduce(jnp.maximum, levels, mine)
            share = jnp.exp2(mine - top)
            shares = [jnp.exp2(level - top) for level in levels]
            whole = share + shares[0] + shares[1] + shares[2]
            acc = o[g] * (share / (total * whole))
            for s in (1, 2, 3):
                acc += orecv[k, s, i, value_rows, :].astype(F32) * (shares[s - 1] / whole)
            merged.append(acc.T.astype(BF))
        one = jnp.concatenate([merged[0], merged[1][:64]], axis=0)
        two = jnp.concatenate([merged[1][64:], merged[2]], axis=0)
        features = jnp.concatenate([one, two, gather(lo, k)], axis=1)
        for c in range(2):
            keep[k, c] = dot(features[c * 96 : c * 96 + 96], wo[...])
        dsend[k] = keep[k, 1 - core].astype(BF)
        send(*d_copy(k))

    def d_copy(k):
        return (dsend.at[k], drecv.at[k], d_s.at[k], d_r.at[k], partner)

    half = D // 2

    def x_copy(i):
        if i < 2:
            return (x0.at[i], ra.at[i], x_s.at[i], x_r.at[i], x_peer(1 if i == 0 else 3))
        k, side = divmod(i - 2, 2)
        return (x12.at[k, side], r1.at[k, side], x_s.at[i], x_r.at[i], x_peer(1 if side == 0 else 3))

    def summed(k):
        remote(*d_copy(k)).wait_recv()
        return keep[k, core] + drecv[k].astype(F32)

    def scatter(k):
        total = summed(k)
        if k == 0:
            for i in range(2):
                x0[i] = total[:, i * half : i * half + half].astype(BF)
                send(*x_copy(i))
        elif k < 3:
            if k == 1:
                for i in range(2):
                    remote(*x_copy(i)).wait_recv()
            for side in range(2):
                mine = total[side * PART : side * PART + PART]
                passing = ra[side, pl.ds((k - 1) * PART, PART), :].astype(F32)
                if side == 0:
                    mine = jnp.concatenate([mine[:, :half] + passing, mine[:, half:]], axis=1)
                else:
                    mine = jnp.concatenate([mine[:, :half], mine[:, half:] + passing], axis=1)
                x12[k - 1, side] = mine.astype(BF)
                send(*x_copy(2 * k + side))
        else:
            for i in range(2, 6):
                remote(*x_copy(i)).wait_recv()
            for part in range(2):
                rows = slice(part * PART, part * PART + PART)
                both = r1[part, 0].astype(F32) + r1[part, 1].astype(F32)
                out[pl.ds(part * PART, PART), :] = (total[rows] + both).astype(BF)

    for i in (10, 11):
        loads[i].wait()
    for k in range(BLOCKS):
        if k == 0:
            wait_queries(0, 1)
        else:
            wait_queries(k, 1 if k % 2 == 0 else 3)
        wait_queries(k, 2)
        attend(k * 10, TILES, lambda i: i, SIDE)
        send_results(k)
        if k < 2:
            relay_queries(k + 2)
        if k > 0:
            merge(k - 1)
            scatter(k - 1)
    merge(3)
    scatter(3)
    for copy in sends:
        copy.wait_send()


def shards(
    tokens,
    norm_gain,
    grid_query_weight,
    grid_key_weight,
    grid_value_weight,
    grid_query_gain,
    grid_key_gain,
    local_query_weight,
    local_key_weight,
    local_value_weight,
    sink_logit,
    grid_out_weight,
    local_out_weight,
):
    row_table, col_table = rope_tables()
    hbm = pl.BlockSpec(memory_space=pl.ANY)
    vmem = pl.BlockSpec(memory_space=pltpu.VMEM)
    smem = pl.BlockSpec(memory_space=pltpu.SMEM)
    dma = pltpu.SemaphoreType.DMA
    return pl.pallas_call(
        kernel,
        out_shape=jax.ShapeDtypeStruct((96, D), BF),
        in_specs=[hbm, vmem, hbm, hbm, hbm, vmem, vmem, hbm, hbm, hbm, smem, hbm, hbm, hbm, vmem],
        out_specs=vmem,
        scratch_shapes=[
            pltpu.VMEM((ROWS, D), BF),
            pltpu.VMEM((ROWS, D), BF),
            pltpu.VMEM((D, 512), BF),
            pltpu.VMEM((D, 512), BF),
            pltpu.VMEM((512, D), BF),
            pltpu.VMEM((2, 16, HEAD), F32),
            pltpu.VMEM((2, ROWS, HEAD), BF),
            pltpu.VMEM((BLOCKS, 3, HEAD, HEAD), BF),
            pltpu.VMEM((48, HEAD, HEAD), BF),
            pltpu.VMEM((SIDE, ROWS, HEAD), BF),
            pltpu.VMEM((SIDE, HEAD + 16, ROWS), BF),
            pltpu.VMEM((48, 1, HEAD), F32),
            pltpu.VMEM((48, 1, HEAD), F32),
            pltpu.VMEM((48, HEAD, HEAD), F32),
            pltpu.VMEM((2, ROWS, 256), F32),
            pltpu.VMEM((2, ROWS, 256), F32),
            pltpu.VMEM((ROWS, 256), BF),
            pltpu.VMEM((ROWS + 2 * WINDOW, HEAD), BF),
            pltpu.VMEM((ROWS + 2 * WINDOW, HEAD), BF),
            pltpu.VMEM((ROWS, 256), BF),
            pltpu.VMEM((BLOCKS, 4, 3, HEAD + 16, HEAD), BF),
            pltpu.VMEM((BLOCKS, 4, 3, HEAD + 16, HEAD), BF),
            pltpu.VMEM((BLOCKS, 2, 96, D), F32),
            pltpu.VMEM((BLOCKS, 96, D), BF),
            pltpu.VMEM((BLOCKS, 96, D), BF),
            pltpu.VMEM((2, 96, D // 2), BF),
            pltpu.VMEM((2, 2, PART, D), BF),
            pltpu.VMEM((2, 96, D // 2), BF),
            pltpu.VMEM((2, 2, PART, D), BF),
            dma((12,)),
            dma((6,)),
            dma((2, 4)),
            dma((BLOCKS, 3)),
            dma((BLOCKS, 4)),
            dma((4,)),
            dma((4,)),
            dma((BLOCKS, 4)),
            dma((BLOCKS, 4)),
            dma((BLOCKS,)),
            dma((BLOCKS,)),
            dma((6,)),
            dma((6,)),
        ],
        compiler_params=pltpu.CompilerParams(
            collective_id=0, has_side_effects=True, vmem_limit_bytes=60 * 2**20
        ),
    )(
        tokens,
        norm_gain.reshape(1, D),
        grid_query_weight,
        grid_key_weight,
        grid_value_weight,
        grid_query_gain.reshape(1, HEAD),
        grid_key_gain.reshape(1, HEAD),
        local_query_weight,
        local_key_weight,
        local_value_weight,
        sink_logit,
        grid_out_weight,
        local_out_weight,
        jnp.asarray(row_table),
        jnp.asarray(col_table),
    )


def solution(mesh):
    in_specs = (
        P("sp", None),
        P(),
        P(None, "tp"),
        P(None, "tp"),
        P(None, "tp"),
        P(),
        P(),
        P(None, "tp"),
        P(None, "tp"),
        P(None, "tp"),
        P("tp"),
        P("tp", None),
        P("tp", None),
    )
    out_specs = P(("sp", "tp"), None)
    return jax.shard_map(shards, mesh=mesh, in_specs=in_specs, out_specs=out_specs, check_vma=False)
```

```python
import functools
import math

import jax
import jax.numpy as jnp
import numpy as np
from jax import lax
from jax.experimental import pallas as pl
from jax.experimental.pallas import tpu as pltpu
from jax.sharding import PartitionSpec as P

D = 2048
HEAD = 128
WINDOW = 128
GRID_W = 64
ROWS = 768
EPSILON = 1e-06
ROPE_BASE = 10000.0
LOG2E = math.log2(math.e)
SCORE = HEAD ** (-0.5) * LOG2E
NSP = 16
SIDE = 4
BLOCKS = 4
CHUNK = 32
PART = 48
EARLY = 40
BF = jnp.bfloat16
F32 = jnp.float32
MESH = pl.DeviceIdType.MESH


def dot(a, b):
    return jnp.dot(a, b, preferred_element_type=F32)


def rope_tables():
    half = HEAD // 2
    inverse = ROPE_BASE ** (-np.arange(0, half, 2, dtype=np.float64) / half)
    sign = np.concatenate([-np.ones(half // 2), np.ones(half // 2)])

    def table(count):
        angle = np.arange(count)[:, None] * np.concatenate([inverse, inverse])
        return np.cos(angle), np.sin(angle) * sign

    rows = np.zeros((2, NSP, 16, HEAD), np.float32)
    cosine, sine = table(NSP * ROWS // GRID_W)
    per = ROWS // GRID_W
    rows[0, :, :per, :half] = cosine.reshape(NSP, per, half)
    rows[1, :, :per, :half] = sine.reshape(NSP, per, half)
    cols = np.zeros((2, GRID_W, HEAD), np.float32)
    cosine, sine = table(GRID_W)
    cols[0, :, half:] = cosine
    cols[1, :, half:] = sine
    return np.ascontiguousarray(rows.transpose(1, 0, 2, 3)), cols


def kernel(
    tokens,
    gain,
    wq,
    wk,
    wv,
    gain_q,
    gain_k,
    lwq,
    lwk,
    lwv,
    sink,
    wog,
    wol,
    row_table,
    col_table,
    out,
    xs,
    xn,
    wkv,
    wqg,
    wl,
    wo,
    rows_tab,
    qr,
    qs,
    qp,
    kall,
    vall,
    m,
    l,
    o,
    s0,
    s1,
    lq,
    lk,
    lv,
    lo,
    osend,
    orecv,
    keep,
    dsend,
    drecv,
    x0,
    x12,
    ra,
    r1,
    in_sem,
    kv_s,
    kv_r,
    q_s,
    q_r,
    h_s,
    h_r,
    o_s,
    o_r,
    d_s,
    d_r,
    x_s,
    x_r,
):
    sp = lax.axis_index("sp")
    tp = lax.axis_index("tp")
    core = lax.rem(tp, 2)
    x = tp // 2
    z = sp // SIDE
    y = lax.rem(sp, SIDE)

    def along_z(d):
        return lax.rem(z + d, SIDE) * SIDE + y

    def along_y(d):
        return z * SIDE + lax.rem(y + d, SIDE)

    def q_peer(d):
        return {"sp": along_z(d) * (1 - core) + along_y(d) * core, "tp": tp}

    def kv_peer(d):
        return {"sp": along_z(d) * core + along_y(d) * (1 - core), "tp": tp}

    def sp_peer(d):
        return {"sp": lax.rem(sp + d, NSP), "tp": tp}

    def x_peer(d):
        return {"sp": sp, "tp": lax.rem(x + d, SIDE) * 2 + core}

    partner = {"sp": sp, "tp": x * 2 + 1 - core}

    def remote(src, dst, send, recv, peer):
        return pltpu.make_async_remote_copy(
            src_ref=src, dst_ref=dst, send_sem=send, recv_sem=recv, device_id=peer, device_id_type=MESH
        )

    def local(src, dst, i):
        return pltpu.make_async_copy(src, dst, in_sem.at[i])

    third = ROWS // 3
    loads = [
        local(tokens.at[pl.ds(0, third)], xs.at[pl.ds(0, third)], 0),
        local(wk, wkv.at[:, pl.ds(0, 128)], 1),
        local(wv, wkv.at[:, pl.ds(128, 128)], 2),
        local(row_table.at[sp], rows_tab, 4),
        local(tokens.at[pl.ds(third, third)], xs.at[pl.ds(third, third)], 5),
        local(tokens.at[pl.ds(2 * third, third)], xs.at[pl.ds(2 * third, third)], 6),
        local(wq, wqg, 3),
        local(lwq, wl.at[:, pl.ds(0, 256)], 7),
        local(lwk, wl.at[:, pl.ds(256, 128)], 8),
        local(lwv, wl.at[:, pl.ds(384, 128)], 9),
        local(wog, wo.at[pl.ds(0, 256)], 10),
        local(wol, wo.at[pl.ds(256, 256)], 11),
    ]
    for load in loads:
        load.start()
    loads = dict(zip((0, 1, 2, 4, 5, 6, 3, 7, 8, 9, 10, 11), loads))

    barrier = pltpu.get_barrier_semaphore()
    peers = [q_peer(1), q_peer(2), q_peer(3), kv_peer(1), kv_peer(3), sp_peer(1), sp_peer(NSP - 1)]
    peers += [x_peer(1), x_peer(3), partner]
    for peer in peers:
        pl.semaphore_signal(barrier, inc=1, device_id=peer, device_id_type=MESH)

    m[...] = jnp.full_like(m, -1e30)
    l[...] = jnp.zeros_like(l)
    o[...] = jnp.zeros_like(o)
    vall[:, pl.ds(HEAD, 16), :] = jnp.ones((SIDE, 16, ROWS), BF)

    lane = lax.broadcasted_iota(jnp.int32, (third, HEAD), 1)
    first_half = lax.rem(lane, 64) < 32

    def norm(r):
        for c in range(third // CHUNK):
            rows = pl.ds(r * third + c * CHUNK, CHUNK)
            squares = jnp.zeros((CHUNK, HEAD), F32)
            for j in range(D // HEAD):
                part = xs[rows, pl.ds(j * HEAD, HEAD)].astype(F32)
                squares += part * part
            factor = lax.rsqrt(jnp.sum(squares, axis=-1, keepdims=True) / D + EPSILON)
            for j in range(D // HEAD):
                cols = pl.ds(j * HEAD, HEAD)
                xn[rows, cols] = (xs[rows, cols].astype(F32) * factor * gain[:, cols]).astype(BF)

    def rope(u, gain_row, r):
        mean = jnp.mean(u * u, axis=-1, keepdims=True)
        u = u * lax.rsqrt(mean + EPSILON) * gain_row
        swapped = jnp.where(first_half, pltpu.roll(u, HEAD - 32, 1), pltpu.roll(u, 32, 1))
        per = third // GRID_W

        def table(which):
            return jnp.concatenate(
                [col_table[which] + rows_tab[which, pl.ds(r * per + i, 1), :] for i in range(per)], axis=0
            )

        return (u * table(0) + swapped * table(1)).astype(BF)

    def project_keys(r):
        rows = pl.ds(r * third, third)
        p = dot(xn[rows, :], wkv[...])
        kall[0, rows, :] = rope(p[:, 0:128], gain_k[...], r)
        vall[0, pl.ds(0, HEAD), rows] = p[:, 128:256].T.astype(BF)

    def project_queries(r):
        rows = pl.ds(r * third, third)
        p = dot(xn[rows, :], wqg[...])
        scaled = gain_q[...] * SCORE
        qr[0, rows, :] = rope(p[:, 0:128], scaled, r)
        qr[1, rows, :] = rope(p[:, 128:256], scaled, r)

    loads[0].wait()
    norm(0)
    for i in (1, 2, 4, 5):
        loads[i].wait()
    norm(1)
    project_keys(0)
    loads[6].wait()
    norm(2)
    project_keys(1)
    project_keys(2)

    pl.semaphore_wait(barrier, len(peers))
    value_rows = pl.ds(0, HEAD)
    sends = []

    def send(*args):
        copy = remote(*args)
        copy.start()
        sends.append(copy)

    def k_copy(slot_from, slot_to, s, d):
        return (kall.at[slot_from], kall.at[slot_to], kv_s.at[s], kv_r.at[0, slot_to], kv_peer(d))

    def v_copy(slot_from, slot_to, s, d):
        return (
            vall.at[slot_from, value_rows],
            vall.at[slot_to, value_rows],
            kv_s.at[s],
            kv_r.at[1, slot_to],
            kv_peer(d),
        )

    k_up, k_down = k_copy(0, 3, 0, 1), k_copy(0, 1, 1, 3)
    v_up, v_down = v_copy(0, 3, 2, 1), v_copy(0, 1, 3, 3)
    for args in (k_up, v_down, k_down, v_up):
        send(*args)
    k_relay, v_relay = k_copy(3, 2, 4, 1), v_copy(1, 2, 5, 3)

    loads[3].wait()
    for r in range(3):
        project_queries(r)
    ahead, behind, across = (lax.rem(x + d, SIDE) * 192 for d in (1, 3, 2))
    own = x * 192
    starts = (
        (across, across + 48, across + 96, across + 144),
        (ahead, behind, ahead + 96, behind + 96),
        (ahead + 48, behind + 48, ahead + 144, behind + 144),
        (own, own + 48, own + 96, own + 144),
    )

    def gather(ref, k):
        return jnp.concatenate([ref[pl.ds(pl.multiple_of(s, 16), PART), :] for s in starts[k]], axis=0)

    for k in range(BLOCKS):
        one, two = gather(qr.at[0], k), gather(qr.at[1], k)
        pieces = (one[:128], jnp.concatenate([one[128:], two[:64]], axis=0), two[64:])
        for i, piece in enumerate(pieces):
            turned = piece.astype(F32).T.astype(BF)
            qs[k, i] = turned
            qp[k * 10 + 9 if i == 2 else EARLY + 2 * k + i] = turned

    place = {2: 0, 1: 3, 3: 6}

    def q_copy(source, k, slot, s, d):
        return (source, qp.at[pl.ds(k * 10 + place[slot], 3)], q_s.at[k, s], q_r.at[k, slot], q_peer(d))

    def send_queries(k):
        send(*q_copy(qs.at[k], k, 3, 0, 1))
        send(*q_copy(qs.at[k], k, 1, 1, 3))

    def relay_queries(k):
        arrived = 3 if k % 2 == 0 else 1
        wait_queries(k, arrived)
        send(*q_copy(qp.at[pl.ds(k * 10 + place[arrived], 3)], k, 2, 2, 4 - arrived))

    def wait_queries(k, slot):
        args = q_copy(qs.at[k], k, slot, 0, 1)
        remote(*args).wait_recv()

    for i in (7, 8, 9):
        loads[i].wait()
    for r in range(3):
        rows = pl.ds(r * third, third)
        p = dot(xn[rows, :], wl[...])
        lq[rows, :] = (p[:, 0:256] * SCORE).astype(BF)
        lk[pl.ds(WINDOW + r * third, third), :] = p[:, 256:384].astype(BF)
        lv[pl.ds(WINDOW + r * third, third), :] = p[:, 384:512].astype(BF)

    def halo(ref, i, low):
        source, target, d = (ROWS, 0, 1) if low else (WINDOW, ROWS + WINDOW, NSP - 1)
        j = 2 * i + (0 if low else 1)
        return (
            ref.at[pl.ds(source, WINDOW)],
            ref.at[pl.ds(target, WINDOW)],
            h_s.at[j],
            h_r.at[j],
            sp_peer(d),
        )

    halos = [halo(ref, i, low) for i, ref in enumerate((lk, lv)) for low in (True, False)]
    for args in halos:
        send(*args)

    def attend(base, tiles, slots, count):
        units = tiles * count // 2

        def where(u):
            halves = []
            for h in range(2):
                index = 2 * u + h
                halves.append((slots(index // tiles), base + 2 * lax.rem(index, tiles)))
            return halves

        def scores(u, ref):
            tops = []
            for h, (t, g) in enumerate(where(u)):
                queries = jnp.concatenate([qp[g], qp[g + 1]], axis=1)
                s = dot(kall[t], queries)
                ref[h] = s
                tops.append(jnp.max(s, axis=0, keepdims=True))
            return tops

        def weigh(u, ref, tops):
            for h, (t, g) in enumerate(where(u)):
                before = jnp.concatenate([m[g], m[g + 1]], axis=1)
                top = jnp.maximum(before, tops[h])
                factor = jnp.exp2(before - top)
                weights = jnp.exp2(ref[h] - top).astype(BF)
                result = dot(vall[t], weights)
                for i in range(2):
                    part = slice(i * 128, i * 128 + 128)
                    m[g + i] = top[:, part]
                    l[g + i] = l[g + i] * factor[:, part] + result[HEAD : HEAD + 1, part]
                    o[g + i] = o[g + i] * factor[:, part] + result[:HEAD, part]

        tops = scores(0, s0)

        def body(i, tops):
            u = 2 * i
            later = scores(u + 1, s1)
            weigh(u, s0, tops)
            tops = scores(jnp.minimum(u + 2, units - 1), s0)
            weigh(u + 1, s1, later)
            return tops

        lax.fori_loop(0, units // 2, body, tops)

    attend(EARLY, 4, lambda i: i * 0, 1)

    send_queries(0)
    send_queries(1)

    for args in halos:
        remote(*args).wait_recv()
    wide = 3 * WINDOW
    row = lax.rem(lax.broadcasted_iota(jnp.int32, (2 * WINDOW, wide), 0), WINDOW)
    col = lax.broadcasted_iota(jnp.int32, (2 * WINDOW, wide), 1)
    near = (col >= row) & (col <= row + 2 * WINDOW)
    sink_rows = jnp.concatenate(
        [jnp.full((WINDOW, 1), sink[0] * LOG2E, F32), jnp.full((WINDOW, 1), sink[1] * LOG2E, F32)], axis=0
    )
    blocks = ROWS // WINDOW

    def banded(n, carry):
        at = pl.multiple_of(n * WINDOW, WINDOW)
        rows = lq[pl.ds(at, WINDOW), :]
        queries = jnp.concatenate([rows[:, :HEAD], rows[:, HEAD:]], axis=0)
        keys = lk[pl.ds(at, wide), :]
        s = lax.dot_general(queries, keys, (((1,), (1,)), ((), ())), preferred_element_type=F32)
        block = sp * blocks + n
        low = jnp.where(block == 0, WINDOW, 0)
        high = jnp.where(block == NSP * blocks - 1, 2 * WINDOW, wide)
        s = jnp.where(near & (col >= low) & (col < high), s, -1e30)
        top = jnp.maximum(jnp.max(s, axis=1, keepdims=True), sink_rows)
        lifted = jnp.exp2(s - top)
        total = jnp.sum(lifted, axis=1, keepdims=True) + jnp.exp2(sink_rows - top)
        result = dot(lifted.astype(BF), lv[pl.ds(at, wide), :]) / total
        lo[pl.ds(at, WINDOW), :] = jnp.concatenate([result[:WINDOW], result[WINDOW:]], axis=1).astype(BF)
        return carry

    lax.fori_loop(0, blocks, banded, 0)

    remote(*k_up).wait_recv()
    send(*k_relay)
    remote(*v_down).wait_recv()
    send(*v_relay)
    for k in (2, 3):
        send_queries(k)
    remote(*k_down).wait_recv()
    remote(*v_up).wait_recv()
    attend(EARLY, 4, lambda i: 1 + 2 * i, 2)
    relay_queries(0)
    remote(*k_relay).wait_recv()
    remote(*v_relay).wait_recv()
    attend(EARLY, 4, lambda i: i * 0 + 2, 1)
    relay_queries(1)

    def packed(g):
        total = l[g]
        level = m[g] + jnp.log2(total)
        high = level.astype(BF)
        rest = level - high.astype(F32)
        mid = rest.astype(BF)
        low = (rest - mid.astype(F32)).astype(BF)
        tail = jnp.concatenate([high, mid, low, jnp.zeros((13, HEAD), BF)], axis=0)
        return jnp.concatenate([(o[g] / total).astype(BF), tail], axis=0)

    def o_copy(k, s):
        return (osend.at[k, s], orecv.at[k, 4 - s], o_s.at[k, s], o_r.at[k, 4 - s], q_peer(s))

    def send_results(k, *targets):
        for s in targets:
            for i in range(3):
                osend[k, s, i] = packed(k * 10 + place[s] + i)
            send(*o_copy(k, s))

    def merge(k):
        for s in (1, 3, 2):
            remote(*o_copy(k, s)).wait_recv()
        merged = []
        for i in range(3):
            g = k * 10 + 9 if i == 2 else EARLY + 2 * k + i
            levels = []
            for s in (1, 2, 3):
                rows = orecv[k, s, i, pl.ds(HEAD, 16), :].astype(F32)
                levels.append(rows[0:1] + rows[1:2] + rows[2:3])
            total = l[g]
            mine = m[g] + jnp.log2(total)
            top = functools.reduce(jnp.maximum, levels, mine)
            share = jnp.exp2(mine - top)
            shares = [jnp.exp2(level - top) for level in levels]
            whole = share + shares[0] + shares[1] + shares[2]
            acc = o[g] * (share / (total * whole))
            for s in (1, 2, 3):
                acc += orecv[k, s, i, value_rows, :].astype(F32) * (shares[s - 1] / whole)
            merged.append(acc.T.astype(BF))
        one = jnp.concatenate([merged[0], merged[1][:64]], axis=0)
        two = jnp.concatenate([merged[1][64:], merged[2]], axis=0)
        features = jnp.concatenate([one, two, gather(lo, k)], axis=1)
        keep[k] = dot(features, wo[...])
        dsend[k] = keep[k, pl.ds(pl.multiple_of((1 - core) * 96, 16), 96), :].astype(BF)
        send(*d_copy(k))

    def d_copy(k):
        return (dsend.at[k], drecv.at[k], d_s.at[k], d_r.at[k], partner)

    half = D // 2

    def x_copy(i):
        if i < 2:
            return (x0.at[i], ra.at[i], x_s.at[i], x_r.at[i], x_peer(1 if i == 0 else 3))
        k, side = divmod(i - 2, 2)
        return (x12.at[k, side], r1.at[k, side], x_s.at[i], x_r.at[i], x_peer(1 if side == 0 else 3))

    def summed(k):
        remote(*d_copy(k)).wait_recv()
        return keep[k, pl.ds(pl.multiple_of(core * 96, 16), 96), :] + drecv[k].astype(F32)

    def scatter(k):
        total = summed(k)
        if k == 0:
            for i in range(2):
                x0[i] = total[:, i * half : i * half + half].astype(BF)
                send(*x_copy(i))
        elif k < 3:
            if k == 1:
                for i in range(2):
                    remote(*x_copy(i)).wait_recv()
            for side in range(2):
                mine = total[side * PART : side * PART + PART]
                passing = ra[side, pl.ds((k - 1) * PART, PART), :].astype(F32)
                if side == 0:
                    mine = jnp.concatenate([mine[:, :half] + passing, mine[:, half:]], axis=1)
                else:
                    mine = jnp.concatenate([mine[:, :half], mine[:, half:] + passing], axis=1)
                x12[k - 1, side] = mine.astype(BF)
                send(*x_copy(2 * k + side))
        else:
            for i in range(2, 6):
                remote(*x_copy(i)).wait_recv()
            for part in range(2):
                rows = slice(part * PART, part * PART + PART)
                both = r1[part, 0].astype(F32) + r1[part, 1].astype(F32)
                out[pl.ds(part * PART, PART), :] = (total[rows] + both).astype(BF)

    for i in (10, 11):
        loads[i].wait()
    for k in range(BLOCKS):
        if k == 0:
            wait_queries(0, 1)
        else:
            wait_queries(k, 1 if k % 2 == 0 else 3)
        wait_queries(k, 2)
        attend(k * 10, 3, lambda i: i, SIDE)
        send_results(k, 2, 1)
        if k < 2:
            relay_queries(k + 2)
        if k > 0:
            merge(k - 1)
        attend(k * 10 + 6, 2, lambda i: i, SIDE)
        send_results(k, 3)
        if k > 0:
            scatter(k - 1)
    merge(3)
    scatter(3)
    for copy in sends:
        copy.wait_send()


def shards(
    tokens,
    norm_gain,
    grid_query_weight,
    grid_key_weight,
    grid_value_weight,
    grid_query_gain,
    grid_key_gain,
    local_query_weight,
    local_key_weight,
    local_value_weight,
    sink_logit,
    grid_out_weight,
    local_out_weight,
):
    row_table, col_table = rope_tables()
    hbm = pl.BlockSpec(memory_space=pl.ANY)
    vmem = pl.BlockSpec(memory_space=pltpu.VMEM)
    smem = pl.BlockSpec(memory_space=pltpu.SMEM)
    dma = pltpu.SemaphoreType.DMA
    return pl.pallas_call(
        kernel,
        out_shape=jax.ShapeDtypeStruct((96, D), BF),
        in_specs=[hbm, vmem, hbm, hbm, hbm, vmem, vmem, hbm, hbm, hbm, smem, hbm, hbm, hbm, vmem],
        out_specs=vmem,
        scratch_shapes=[
            pltpu.VMEM((ROWS, D), BF),
            pltpu.VMEM((ROWS, D), BF),
            pltpu.VMEM((D, 256), BF),
            pltpu.VMEM((D, 256), BF),
            pltpu.VMEM((D, 512), BF),
            pltpu.VMEM((512, D), BF),
            pltpu.VMEM((2, 16, HEAD), F32),
            pltpu.VMEM((2, ROWS, HEAD), BF),
            pltpu.VMEM((BLOCKS, 3, HEAD, HEAD), BF),
            pltpu.VMEM((48, HEAD, HEAD), BF),
            pltpu.VMEM((SIDE, ROWS, HEAD), BF),
            pltpu.VMEM((SIDE, HEAD + 16, ROWS), BF),
            pltpu.VMEM((48, 1, HEAD), F32),
            pltpu.VMEM((48, 1, HEAD), F32),
            pltpu.VMEM((48, HEAD, HEAD), F32),
            pltpu.VMEM((2, ROWS, 256), F32),
            pltpu.VMEM((2, ROWS, 256), F32),
            pltpu.VMEM((ROWS, 256), BF),
            pltpu.VMEM((ROWS + 2 * WINDOW, HEAD), BF),
            pltpu.VMEM((ROWS + 2 * WINDOW, HEAD), BF),
            pltpu.VMEM((ROWS, 256), BF),
            pltpu.VMEM((BLOCKS, 4, 3, HEAD + 16, HEAD), BF),
            pltpu.VMEM((BLOCKS, 4, 3, HEAD + 16, HEAD), BF),
            pltpu.VMEM((BLOCKS, 192, D), F32),
            pltpu.VMEM((BLOCKS, 96, D), BF),
            pltpu.VMEM((BLOCKS, 96, D), BF),
            pltpu.VMEM((2, 96, D // 2), BF),
            pltpu.VMEM((2, 2, PART, D), BF),
            pltpu.VMEM((2, 96, D // 2), BF),
            pltpu.VMEM((2, 2, PART, D), BF),
            dma((12,)),
            dma((6,)),
            dma((2, 4)),
            dma((BLOCKS, 3)),
            dma((BLOCKS, 4)),
            dma((4,)),
            dma((4,)),
            dma((BLOCKS, 4)),
            dma((BLOCKS, 4)),
            dma((BLOCKS,)),
            dma((BLOCKS,)),
            dma((6,)),
            dma((6,)),
        ],
        compiler_params=pltpu.CompilerParams(
            collective_id=0, has_side_effects=True, vmem_limit_bytes=60 * 2**20
        ),
    )(
        tokens,
        norm_gain.reshape(1, D),
        grid_query_weight,
        grid_key_weight,
        grid_value_weight,
        grid_query_gain.reshape(1, HEAD),
        grid_key_gain.reshape(1, HEAD),
        local_query_weight,
        local_key_weight,
        local_value_weight,
        sink_logit,
        grid_out_weight,
        local_out_weight,
        jnp.asarray(row_table),
        jnp.asarray(col_table),
    )


def solution(mesh):
    in_specs = (
        P("sp", None),
        P(),
        P(None, "tp"),
        P(None, "tp"),
        P(None, "tp"),
        P(),
        P(),
        P(None, "tp"),
        P(None, "tp"),
        P(None, "tp"),
        P("tp"),
        P("tp", None),
        P("tp", None),
    )
    out_specs = P(("sp", "tp"), None)
    return jax.shard_map(shards, mesh=mesh, in_specs=in_specs, out_specs=out_specs, check_vma=False)
```

```python
import functools
import math

import jax
import jax.numpy as jnp
import numpy as np
from jax import lax
from jax.experimental import pallas as pl
from jax.experimental.pallas import tpu as pltpu
from jax.sharding import PartitionSpec as P

D = 2048
HEAD = 128
WINDOW = 128
GRID_W = 64
ROWS = 768
EPSILON = 1e-06
ROPE_BASE = 10000.0
LOG2E = math.log2(math.e)
SCORE = HEAD ** (-0.5) * LOG2E
NSP = 16
SIDE = 4
BLOCKS = 4
CHUNK = 32
PART = 48
EARLY = 40
BF = jnp.bfloat16
F32 = jnp.float32
MESH = pl.DeviceIdType.MESH


def dot(a, b):
    return jnp.dot(a, b, preferred_element_type=F32)


def rope_tables():
    half = HEAD // 2
    inverse = ROPE_BASE ** (-np.arange(0, half, 2, dtype=np.float64) / half)
    sign = np.concatenate([-np.ones(half // 2), np.ones(half // 2)])

    def table(count):
        angle = np.arange(count)[:, None] * np.concatenate([inverse, inverse])
        return np.cos(angle), np.sin(angle) * sign

    rows = np.zeros((2, NSP, 16, HEAD), np.float32)
    cosine, sine = table(NSP * ROWS // GRID_W)
    per = ROWS // GRID_W
    rows[0, :, :per, :half] = cosine.reshape(NSP, per, half)
    rows[1, :, :per, :half] = sine.reshape(NSP, per, half)
    cols = np.zeros((2, GRID_W, HEAD), np.float32)
    cosine, sine = table(GRID_W)
    cols[0, :, half:] = cosine
    cols[1, :, half:] = sine
    return np.ascontiguousarray(rows.transpose(1, 0, 2, 3)), cols


def kernel(
    tokens,
    gain,
    wq,
    wk,
    wv,
    gain_q,
    gain_k,
    lwq,
    lwk,
    lwv,
    sink,
    wog,
    wol,
    row_table,
    col_table,
    out,
    xs,
    xn,
    wkv,
    wqg,
    wl,
    wo,
    rows_tab,
    qr,
    qs,
    qp,
    kall,
    vall,
    m,
    l,
    o,
    s0,
    s1,
    lq,
    lk,
    lv,
    lo,
    osend,
    orecv,
    keep,
    dsend,
    drecv,
    x0,
    x12,
    ra,
    r1,
    in_sem,
    kv_s,
    kv_r,
    q_s,
    q_r,
    h_s,
    h_r,
    o_s,
    o_r,
    d_s,
    d_r,
    x_s,
    x_r,
):
    sp = lax.axis_index("sp")
    tp = lax.axis_index("tp")
    core = lax.rem(tp, 2)
    x = tp // 2
    z = sp // SIDE
    y = lax.rem(sp, SIDE)

    def along_z(d):
        return lax.rem(z + d, SIDE) * SIDE + y

    def along_y(d):
        return z * SIDE + lax.rem(y + d, SIDE)

    def q_peer(d):
        return {"sp": along_z(d) * (1 - core) + along_y(d) * core, "tp": tp}

    def kv_peer(d):
        return {"sp": along_z(d) * core + along_y(d) * (1 - core), "tp": tp}

    def sp_peer(d):
        return {"sp": lax.rem(sp + d, NSP), "tp": tp}

    def x_peer(d):
        return {"sp": sp, "tp": lax.rem(x + d, SIDE) * 2 + core}

    partner = {"sp": sp, "tp": x * 2 + 1 - core}

    def remote(src, dst, send, recv, peer):
        return pltpu.make_async_remote_copy(
            src_ref=src, dst_ref=dst, send_sem=send, recv_sem=recv, device_id=peer, device_id_type=MESH
        )

    def local(src, dst, i):
        return pltpu.make_async_copy(src, dst, in_sem.at[i])

    third = ROWS // 3
    loads = [
        local(tokens.at[pl.ds(0, third)], xs.at[pl.ds(0, third)], 0),
        local(wk, wkv.at[:, pl.ds(0, 128)], 1),
        local(wv, wkv.at[:, pl.ds(128, 128)], 2),
        local(row_table.at[sp], rows_tab, 4),
        local(tokens.at[pl.ds(third, third)], xs.at[pl.ds(third, third)], 5),
        local(tokens.at[pl.ds(2 * third, third)], xs.at[pl.ds(2 * third, third)], 6),
        local(wq, wqg, 3),
        local(lwq, wl.at[:, pl.ds(0, 256)], 7),
        local(lwk, wl.at[:, pl.ds(256, 128)], 8),
        local(lwv, wl.at[:, pl.ds(384, 128)], 9),
        local(wog, wo.at[pl.ds(0, 256)], 10),
        local(wol, wo.at[pl.ds(256, 256)], 11),
    ]
    loads = dict(zip((0, 1, 2, 4, 5, 6, 3, 7, 8, 9, 10, 11), loads))
    for i in (0, 1, 2, 4, 5, 6):
        loads[i].start()

    barrier = pltpu.get_barrier_semaphore()
    peers = [q_peer(1), q_peer(2), q_peer(3), kv_peer(1), kv_peer(3), sp_peer(1), sp_peer(NSP - 1)]
    peers += [x_peer(1), x_peer(3), partner]
    for peer in peers:
        pl.semaphore_signal(barrier, inc=1, device_id=peer, device_id_type=MESH)

    m[...] = jnp.full_like(m, -1e30)
    l[...] = jnp.zeros_like(l)
    o[...] = jnp.zeros_like(o)
    vall[:, pl.ds(HEAD, 16), :] = jnp.ones((SIDE, 16, ROWS), BF)

    lane = lax.broadcasted_iota(jnp.int32, (third, HEAD), 1)
    first_half = lax.rem(lane, 64) < 32

    def norm(r):
        for c in range(third // CHUNK):
            rows = pl.ds(r * third + c * CHUNK, CHUNK)
            squares = jnp.zeros((CHUNK, HEAD), F32)
            for j in range(D // HEAD):
                part = xs[rows, pl.ds(j * HEAD, HEAD)].astype(F32)
                squares += part * part
            factor = lax.rsqrt(jnp.sum(squares, axis=-1, keepdims=True) / D + EPSILON)
            for j in range(D // HEAD):
                cols = pl.ds(j * HEAD, HEAD)
                xn[rows, cols] = (xs[rows, cols].astype(F32) * factor * gain[:, cols]).astype(BF)

    def rope(u, gain_row, r):
        mean = jnp.mean(u * u, axis=-1, keepdims=True)
        u = u * lax.rsqrt(mean + EPSILON) * gain_row
        swapped = jnp.where(first_half, pltpu.roll(u, HEAD - 32, 1), pltpu.roll(u, 32, 1))
        per = third // GRID_W

        def table(which):
            return jnp.concatenate(
                [col_table[which] + rows_tab[which, pl.ds(r * per + i, 1), :] for i in range(per)], axis=0
            )

        return (u * table(0) + swapped * table(1)).astype(BF)

    def project_keys(r):
        rows = pl.ds(r * third, third)
        p = dot(xn[rows, :], wkv[...])
        kall[0, rows, :] = rope(p[:, 0:128], gain_k[...], r)
        vall[0, pl.ds(0, HEAD), rows] = p[:, 128:256].T.astype(BF)

    def project_queries(r):
        rows = pl.ds(r * third, third)
        p = dot(xn[rows, :], wqg[...])
        scaled = gain_q[...] * SCORE
        qr[0, rows, :] = rope(p[:, 0:128], scaled, r)
        qr[1, rows, :] = rope(p[:, 128:256], scaled, r)

    loads[0].wait()
    loads[3].start()
    norm(0)
    for i in (1, 2, 4, 5):
        loads[i].wait()
    for i in (7, 8, 9, 10, 11):
        loads[i].start()
    norm(1)
    project_keys(0)
    loads[6].wait()
    norm(2)
    project_keys(1)
    project_keys(2)

    pl.semaphore_wait(barrier, len(peers))
    value_rows = pl.ds(0, HEAD)
    sends = []

    def send(*args):
        copy = remote(*args)
        copy.start()
        sends.append(copy)

    def k_copy(slot_from, slot_to, s, d):
        return (kall.at[slot_from], kall.at[slot_to], kv_s.at[s], kv_r.at[0, slot_to], kv_peer(d))

    def v_copy(slot_from, slot_to, s, d):
        return (
            vall.at[slot_from, value_rows],
            vall.at[slot_to, value_rows],
            kv_s.at[s],
            kv_r.at[1, slot_to],
            kv_peer(d),
        )

    k_up, k_down = k_copy(0, 3, 0, 1), k_copy(0, 1, 1, 3)
    v_up, v_down = v_copy(0, 3, 2, 1), v_copy(0, 1, 3, 3)
    for args in (k_up, v_down, k_down, v_up):
        send(*args)
    k_relay, v_relay = k_copy(3, 2, 4, 1), v_copy(1, 2, 5, 3)

    loads[3].wait()
    for r in range(3):
        project_queries(r)
    ahead, behind, across = (lax.rem(x + d, SIDE) * 192 for d in (1, 3, 2))
    own = x * 192
    starts = (
        (across, across + 48, across + 96, across + 144),
        (ahead, behind, ahead + 96, behind + 96),
        (ahead + 48, behind + 48, ahead + 144, behind + 144),
        (own, own + 48, own + 96, own + 144),
    )

    def gather(ref, k):
        return jnp.concatenate([ref[pl.ds(pl.multiple_of(s, 16), PART), :] for s in starts[k]], axis=0)

    for k in range(BLOCKS):
        one, two = gather(qr.at[0], k), gather(qr.at[1], k)
        pieces = (one[:128], jnp.concatenate([one[128:], two[:64]], axis=0), two[64:])
        for i, piece in enumerate(pieces):
            turned = piece.astype(F32).T.astype(BF)
            qs[k, i] = turned
            qp[k * 10 + 9 if i == 2 else EARLY + 2 * k + i] = turned

    place = {2: 0, 1: 3, 3: 6}

    def q_copy(source, k, slot, s, d):
        return (source, qp.at[pl.ds(k * 10 + place[slot], 3)], q_s.at[k, s], q_r.at[k, slot], q_peer(d))

    def send_queries(k):
        send(*q_copy(qs.at[k], k, 3, 0, 1))
        send(*q_copy(qs.at[k], k, 1, 1, 3))

    def relay_queries(k):
        arrived = 3 if k % 2 == 0 else 1
        wait_queries(k, arrived)
        send(*q_copy(qp.at[pl.ds(k * 10 + place[arrived], 3)], k, 2, 2, 4 - arrived))

    def wait_queries(k, slot):
        args = q_copy(qs.at[k], k, slot, 0, 1)
        remote(*args).wait_recv()

    for k in range(BLOCKS):
        send_queries(k)

    for i in (7, 8, 9):
        loads[i].wait()
    for r in range(3):
        rows = pl.ds(r * third, third)
        p = dot(xn[rows, :], wl[...])
        lq[rows, :] = (p[:, 0:256] * SCORE).astype(BF)
        lk[pl.ds(WINDOW + r * third, third), :] = p[:, 256:384].astype(BF)
        lv[pl.ds(WINDOW + r * third, third), :] = p[:, 384:512].astype(BF)

    def halo(ref, i, low):
        source, target, d = (ROWS, 0, 1) if low else (WINDOW, ROWS + WINDOW, NSP - 1)
        j = 2 * i + (0 if low else 1)
        return (
            ref.at[pl.ds(source, WINDOW)],
            ref.at[pl.ds(target, WINDOW)],
            h_s.at[j],
            h_r.at[j],
            sp_peer(d),
        )

    halos = [halo(ref, i, low) for i, ref in enumerate((lk, lv)) for low in (True, False)]
    for args in halos:
        send(*args)

    def attend(base, tiles, slots, count, tops=None, following=None):
        units = tiles * count // 2

        def where(u):
            halves = []
            for h in range(2):
                index = 2 * u + h
                halves.append((slots(index // tiles), base + lax.rem(index, tiles)))
            return halves

        def scores(halves, ref):
            tops = []
            for h, (t, g) in enumerate(halves):
                queries = jnp.concatenate([qp[2 * g], qp[2 * g + 1]], axis=1)
                s = dot(kall[t], queries)
                ref[h] = s
                tops.append(jnp.max(s, axis=0, keepdims=True))
            return tops

        def weigh(halves, ref, tops):
            for h, (t, g) in enumerate(halves):
                before = m[g]
                top = jnp.maximum(before, tops[h])
                factor = jnp.exp2(before - top)
                weights = jnp.exp2(ref[h] - top).astype(BF)
                result = dot(vall[t], weights)
                m[g] = top
                l[g] = l[g] * factor + result[HEAD : HEAD + 1]
                o[g] = o[g] * factor + result[:HEAD]

        if tops is None:
            tops = scores(where(0), s0)

        def body(i, tops):
            u = 2 * i
            later = scores(where(u + 1), s1)
            weigh(where(u), s0, tops)
            after = where(jnp.minimum(u + 2, units - 1))
            if following is not None:
                last = (i + 1) // (units // 2)
                after = [
                    (t * (1 - last) + ft * last, g * (1 - last) + fg * last)
                    for (t, g), (ft, fg) in zip(after, following)
                ]
            tops = scores(after, s0)
            weigh(where(u + 1), s1, later)
            return tops

        return lax.fori_loop(0, units // 2, body, tops)

    attend(EARLY // 2, 4, lambda i: i * 0, 1)

    wide = 3 * WINDOW
    row = lax.rem(lax.broadcasted_iota(jnp.int32, (2 * WINDOW, wide), 0), WINDOW)
    col = lax.broadcasted_iota(jnp.int32, (2 * WINDOW, wide), 1)
    near = (col >= row) & (col <= row + 2 * WINDOW)
    sink_rows = jnp.concatenate(
        [jnp.full((WINDOW, 1), sink[0] * LOG2E, F32), jnp.full((WINDOW, 1), sink[1] * LOG2E, F32)], axis=0
    )
    blocks = ROWS // WINDOW

    def banded(n, carry):
        at = pl.multiple_of(n * WINDOW, WINDOW)
        rows = lq[pl.ds(at, WINDOW), :]
        queries = jnp.concatenate([rows[:, :HEAD], rows[:, HEAD:]], axis=0)
        keys = lk[pl.ds(at, wide), :]
        s = lax.dot_general(queries, keys, (((1,), (1,)), ((), ())), preferred_element_type=F32)
        block = sp * blocks + n
        low = jnp.where(block == 0, WINDOW, 0)
        high = jnp.where(block == NSP * blocks - 1, 2 * WINDOW, wide)
        s = jnp.where(near & (col >= low) & (col < high), s, -1e30)
        top = jnp.maximum(jnp.max(s, axis=1, keepdims=True), sink_rows)
        lifted = jnp.exp2(s - top)
        total = jnp.sum(lifted, axis=1, keepdims=True) + jnp.exp2(sink_rows - top)
        result = dot(lifted.astype(BF), lv[pl.ds(at, wide), :]) / total
        lo[pl.ds(at, WINDOW), :] = jnp.concatenate([result[:WINDOW], result[WINDOW:]], axis=1).astype(BF)
        return carry

    lax.fori_loop(1, blocks - 1, banded, 0)

    remote(*k_up).wait_recv()
    send(*k_relay)
    remote(*v_down).wait_recv()
    send(*v_relay)
    remote(*k_down).wait_recv()
    remote(*v_up).wait_recv()
    attend(EARLY // 2, 4, lambda i: 1 + 2 * i, 2)
    relay_queries(0)
    relay_queries(1)
    for args in halos:
        remote(*args).wait_recv()
    lax.fori_loop(0, 2, lambda i, carry: banded(i * (blocks - 1), carry), 0)
    remote(*k_relay).wait_recv()
    remote(*v_relay).wait_recv()
    attend(EARLY // 2, 4, lambda i: i * 0 + 2, 1)
    relay_queries(2)
    relay_queries(3)

    def state(g):
        lanes = pl.ds(g % 2 * HEAD, HEAD)
        return m[g // 2, :, lanes], l[g // 2, :, lanes], o[g // 2, :, lanes]

    def packed(g):
        top, total, result = state(g)
        level = top + jnp.log2(total)
        high = level.astype(BF)
        rest = level - high.astype(F32)
        mid = rest.astype(BF)
        low = (rest - mid.astype(F32)).astype(BF)
        tail = jnp.concatenate([high, mid, low, jnp.zeros((13, HEAD), BF)], axis=0)
        return jnp.concatenate([(result * (1.0 / total)).astype(BF), tail], axis=0)

    def o_copy(k, s):
        return (osend.at[k, s], orecv.at[k, 4 - s], o_s.at[k, s], o_r.at[k, 4 - s], q_peer(s))

    def send_results(k, *targets):
        for s in targets:
            for i in range(3):
                osend[k, s, i] = packed(k * 10 + place[s] + i)
            send(*o_copy(k, s))

    def merge(k):
        for s in (1, 3, 2):
            remote(*o_copy(k, s)).wait_recv()
        merged = []
        for i in range(3):
            g = k * 10 + 9 if i == 2 else EARLY + 2 * k + i
            levels = []
            for s in (1, 2, 3):
                rows = orecv[k, s, i, pl.ds(HEAD, 16), :].astype(F32)
                levels.append(rows[0:1] + rows[1:2] + rows[2:3])
            highest, total, result = state(g)
            mine = highest + jnp.log2(total)
            top = functools.reduce(jnp.maximum, levels, mine)
            share = jnp.exp2(mine - top)
            shares = [jnp.exp2(level - top) for level in levels]
            whole = share + shares[0] + shares[1] + shares[2]
            acc = result * (share / (total * whole))
            for s in (1, 2, 3):
                acc += orecv[k, s, i, value_rows, :].astype(F32) * (shares[s - 1] / whole)
            merged.append(acc.T.astype(BF))
        one = jnp.concatenate([merged[0], merged[1][:64]], axis=0)
        two = jnp.concatenate([merged[1][64:], merged[2]], axis=0)
        features = jnp.concatenate([one, two, gather(lo, k)], axis=1)
        keep[k] = dot(features, wo[...])
        dsend[k] = keep[k, pl.ds(pl.multiple_of((1 - core) * 96, 16), 96), :].astype(BF)
        send(*d_copy(k))

    def d_copy(k):
        return (dsend.at[k], drecv.at[k], d_s.at[k], d_r.at[k], partner)

    half = D // 2

    def x_copy(i):
        if i < 2:
            return (x0.at[i], ra.at[i], x_s.at[i], x_r.at[i], x_peer(1 if i == 0 else 3))
        k, side = divmod(i - 2, 2)
        return (x12.at[k, side], r1.at[k, side], x_s.at[i], x_r.at[i], x_peer(1 if side == 0 else 3))

    def summed(k):
        remote(*d_copy(k)).wait_recv()
        return keep[k, pl.ds(pl.multiple_of(core * 96, 16), 96), :] + drecv[k].astype(F32)

    def scatter(k):
        total = summed(k)
        if k == 0:
            for i in range(2):
                x0[i] = total[:, i * half : i * half + half].astype(BF)
                send(*x_copy(i))
        elif k < 3:
            if k == 1:
                for i in range(2):
                    remote(*x_copy(i)).wait_recv()
            for side in range(2):
                mine = total[side * PART : side * PART + PART]
                passing = ra[side, pl.ds((k - 1) * PART, PART), :].astype(F32)
                if side == 0:
                    mine = jnp.concatenate([mine[:, :half] + passing, mine[:, half:]], axis=1)
                else:
                    mine = jnp.concatenate([mine[:, :half], mine[:, half:] + passing], axis=1)
                x12[k - 1, side] = mine.astype(BF)
                send(*x_copy(2 * k + side))
        else:
            for i in range(2, 6):
                remote(*x_copy(i)).wait_recv()
            for part in range(2):
                rows = slice(part * PART, part * PART + PART)
                both = r1[part, 0].astype(F32) + r1[part, 1].astype(F32)
                out[pl.ds(part * PART, PART), :] = (total[rows] + both).astype(BF)

    for i in (10, 11):
        loads[i].wait()
    def wait_block(k):
        wait_queries(k, 1 if k % 2 == 0 else 3)
        wait_queries(k, 2)

    wait_block(0)
    tops = None
    for k in range(BLOCKS):
        tops = attend(k * 5, 3, lambda i: i, SIDE, tops, [(0, k * 5 + 3), (0, k * 5 + 4)])
        send_results(k, 2, 1)
        if k > 0:
            merge(k - 1)
        following = None
        if k + 1 < BLOCKS:
            wait_block(k + 1)
            following = [(0, k * 5 + 5), (0, k * 5 + 6)]
        tops = attend(k * 5 + 3, 2, lambda i: i, SIDE, tops, following)
        send_results(k, 3)
        if k > 0:
            scatter(k - 1)
    merge(3)
    scatter(3)
    for copy in sends:
        copy.wait_send()


def shards(
    tokens,
    norm_gain,
    grid_query_weight,
    grid_key_weight,
    grid_value_weight,
    grid_query_gain,
    grid_key_gain,
    local_query_weight,
    local_key_weight,
    local_value_weight,
    sink_logit,
    grid_out_weight,
    local_out_weight,
):
    row_table, col_table = rope_tables()
    hbm = pl.BlockSpec(memory_space=pl.ANY)
    vmem = pl.BlockSpec(memory_space=pltpu.VMEM)
    smem = pl.BlockSpec(memory_space=pltpu.SMEM)
    dma = pltpu.SemaphoreType.DMA
    return pl.pallas_call(
        kernel,
        out_shape=jax.ShapeDtypeStruct((96, D), BF),
        in_specs=[hbm, vmem, hbm, hbm, hbm, vmem, vmem, hbm, hbm, hbm, smem, hbm, hbm, hbm, vmem],
        out_specs=vmem,
        scratch_shapes=[
            pltpu.VMEM((ROWS, D), BF),
            pltpu.VMEM((ROWS, D), BF),
            pltpu.VMEM((D, 256), BF),
            pltpu.VMEM((D, 256), BF),
            pltpu.VMEM((D, 512), BF),
            pltpu.VMEM((512, D), BF),
            pltpu.VMEM((2, 16, HEAD), F32),
            pltpu.VMEM((2, ROWS, HEAD), BF),
            pltpu.VMEM((BLOCKS, 3, HEAD, HEAD), BF),
            pltpu.VMEM((48, HEAD, HEAD), BF),
            pltpu.VMEM((SIDE, ROWS, HEAD), BF),
            pltpu.VMEM((SIDE, HEAD + 16, ROWS), BF),
            pltpu.VMEM((24, 1, 2 * HEAD), F32),
            pltpu.VMEM((24, 1, 2 * HEAD), F32),
            pltpu.VMEM((24, HEAD, 2 * HEAD), F32),
            pltpu.VMEM((2, ROWS, 256), F32),
            pltpu.VMEM((2, ROWS, 256), F32),
            pltpu.VMEM((ROWS, 256), BF),
            pltpu.VMEM((ROWS + 2 * WINDOW, HEAD), BF),
            pltpu.VMEM((ROWS + 2 * WINDOW, HEAD), BF),
            pltpu.VMEM((ROWS, 256), BF),
            pltpu.VMEM((BLOCKS, 4, 3, HEAD + 16, HEAD), BF),
            pltpu.VMEM((BLOCKS, 4, 3, HEAD + 16, HEAD), BF),
            pltpu.VMEM((BLOCKS, 192, D), F32),
            pltpu.VMEM((BLOCKS, 96, D), BF),
            pltpu.VMEM((BLOCKS, 96, D), BF),
            pltpu.VMEM((2, 96, D // 2), BF),
            pltpu.VMEM((2, 2, PART, D), BF),
            pltpu.VMEM((2, 96, D // 2), BF),
            pltpu.VMEM((2, 2, PART, D), BF),
            dma((12,)),
            dma((6,)),
            dma((2, 4)),
            dma((BLOCKS, 3)),
            dma((BLOCKS, 4)),
            dma((4,)),
            dma((4,)),
            dma((BLOCKS, 4)),
            dma((BLOCKS, 4)),
            dma((BLOCKS,)),
            dma((BLOCKS,)),
            dma((6,)),
            dma((6,)),
        ],
        compiler_params=pltpu.CompilerParams(
            collective_id=0, has_side_effects=True, vmem_limit_bytes=60 * 2**20
        ),
    )(
        tokens,
        norm_gain.reshape(1, D),
        grid_query_weight,
        grid_key_weight,
        grid_value_weight,
        grid_query_gain.reshape(1, HEAD),
        grid_key_gain.reshape(1, HEAD),
        local_query_weight,
        local_key_weight,
        local_value_weight,
        sink_logit,
        grid_out_weight,
        local_out_weight,
        jnp.asarray(row_table),
        jnp.asarray(col_table),
    )


def solution(mesh):
    in_specs = (
        P("sp", None),
        P(),
        P(None, "tp"),
        P(None, "tp"),
        P(None, "tp"),
        P(),
        P(),
        P(None, "tp"),
        P(None, "tp"),
        P(None, "tp"),
        P("tp"),
        P("tp", None),
        P("tp", None),
    )
    out_specs = P(("sp", "tp"), None)
    return jax.shard_map(shards, mesh=mesh, in_specs=in_specs, out_specs=out_specs, check_vma=False)
```

```python
import functools
import math

import jax
import jax.numpy as jnp
import numpy as np
from jax import lax
from jax.experimental import pallas as pl
from jax.experimental.pallas import tpu as pltpu
from jax.sharding import PartitionSpec as P

D = 2048
HEAD = 128
WINDOW = 128
GRID_W = 64
ROWS = 768
EPSILON = 1e-06
ROPE_BASE = 10000.0
LOG2E = math.log2(math.e)
SCORE = HEAD ** (-0.5) * LOG2E
NSP = 16
SIDE = 4
BLOCKS = 4
CHUNK = 32
PART = 48
EARLY = 40
BF = jnp.bfloat16
F32 = jnp.float32
MESH = pl.DeviceIdType.MESH


def dot(a, b):
    return jnp.dot(a, b, preferred_element_type=F32)


def rope_tables():
    half = HEAD // 2
    inverse = ROPE_BASE ** (-np.arange(0, half, 2, dtype=np.float64) / half)
    sign = np.concatenate([-np.ones(half // 2), np.ones(half // 2)])

    def table(count):
        angle = np.arange(count)[:, None] * np.concatenate([inverse, inverse])
        return np.cos(angle), np.sin(angle) * sign

    rows = np.zeros((2, NSP, 16, HEAD), np.float32)
    cosine, sine = table(NSP * ROWS // GRID_W)
    per = ROWS // GRID_W
    rows[0, :, :per, :half] = cosine.reshape(NSP, per, half)
    rows[1, :, :per, :half] = sine.reshape(NSP, per, half)
    cols = np.zeros((2, GRID_W, HEAD), np.float32)
    cosine, sine = table(GRID_W)
    cols[0, :, half:] = cosine
    cols[1, :, half:] = sine
    return np.ascontiguousarray(rows.transpose(1, 0, 2, 3)), cols


def kernel(
    tokens,
    gain,
    wq,
    wk,
    wv,
    gain_q,
    gain_k,
    lwq,
    lwk,
    lwv,
    sink,
    wog,
    wol,
    row_table,
    col_table,
    out,
    xs,
    xn,
    wkv,
    wqg,
    wl,
    wo,
    rows_tab,
    qr,
    qs,
    qp,
    kall,
    vall,
    m,
    l,
    o,
    s0,
    s1,
    lq,
    lk,
    lv,
    lo,
    osend,
    orecv,
    keep,
    dsend,
    drecv,
    x0,
    x12,
    ra,
    r1,
    in_sem,
    kv_s,
    kv_r,
    q_s,
    q_r,
    h_s,
    h_r,
    o_s,
    o_r,
    d_s,
    d_r,
    x_s,
    x_r,
):
    sp = lax.axis_index("sp")
    tp = lax.axis_index("tp")
    core = lax.rem(tp, 2)
    x = tp // 2
    z = sp // SIDE
    y = lax.rem(sp, SIDE)

    def along_z(d):
        return lax.rem(z + d, SIDE) * SIDE + y

    def along_y(d):
        return z * SIDE + lax.rem(y + d, SIDE)

    def q_peer(d):
        return {"sp": along_z(d) * (1 - core) + along_y(d) * core, "tp": tp}

    def kv_peer(d):
        return {"sp": along_z(d) * core + along_y(d) * (1 - core), "tp": tp}

    def sp_peer(d):
        return {"sp": lax.rem(sp + d, NSP), "tp": tp}

    def x_peer(d):
        return {"sp": sp, "tp": lax.rem(x + d, SIDE) * 2 + core}

    partner = {"sp": sp, "tp": x * 2 + 1 - core}

    def remote(src, dst, send, recv, peer):
        return pltpu.make_async_remote_copy(
            src_ref=src, dst_ref=dst, send_sem=send, recv_sem=recv, device_id=peer, device_id_type=MESH
        )

    def local(src, dst, i):
        return pltpu.make_async_copy(src, dst, in_sem.at[i])

    third = ROWS // 3
    loads = [
        local(tokens.at[pl.ds(0, third)], xs.at[pl.ds(0, third)], 0),
        local(wk, wkv.at[:, pl.ds(0, 128)], 1),
        local(wv, wkv.at[:, pl.ds(128, 128)], 2),
        local(row_table.at[sp], rows_tab, 4),
        local(tokens.at[pl.ds(third, third)], xs.at[pl.ds(third, third)], 5),
        local(tokens.at[pl.ds(2 * third, third)], xs.at[pl.ds(2 * third, third)], 6),
        local(wq, wqg, 3),
        local(lwq, wl.at[:, pl.ds(0, 256)], 7),
        local(lwk, wl.at[:, pl.ds(256, 128)], 8),
        local(lwv, wl.at[:, pl.ds(384, 128)], 9),
        local(wog, wo.at[pl.ds(0, 256)], 10),
        local(wol, wo.at[pl.ds(256, 256)], 11),
    ]
    loads = dict(zip((0, 1, 2, 4, 5, 6, 3, 7, 8, 9, 10, 11), loads))
    for i in (0, 1, 2, 4, 5, 6):
        loads[i].start()

    barrier = pltpu.get_barrier_semaphore()
    peers = [q_peer(1), q_peer(2), q_peer(3), kv_peer(1), kv_peer(3), sp_peer(1), sp_peer(NSP - 1)]
    peers += [x_peer(1), x_peer(3), partner]
    for peer in peers:
        pl.semaphore_signal(barrier, inc=1, device_id=peer, device_id_type=MESH)

    m[...] = jnp.full_like(m, -1e30)
    l[...] = jnp.zeros_like(l)
    o[...] = jnp.zeros_like(o)
    vall[:, pl.ds(HEAD, 16), :] = jnp.ones((SIDE, 16, ROWS), BF)

    lane = lax.broadcasted_iota(jnp.int32, (third, HEAD), 1)
    first_half = lax.rem(lane, 64) < 32

    def norm(r):
        for c in range(third // CHUNK):
            rows = pl.ds(r * third + c * CHUNK, CHUNK)
            squares = jnp.zeros((CHUNK, HEAD), F32)
            for j in range(D // HEAD):
                part = xs[rows, pl.ds(j * HEAD, HEAD)].astype(F32)
                squares += part * part
            factor = lax.rsqrt(jnp.sum(squares, axis=-1, keepdims=True) / D + EPSILON)
            for j in range(D // HEAD):
                cols = pl.ds(j * HEAD, HEAD)
                xn[rows, cols] = (xs[rows, cols].astype(F32) * factor * gain[:, cols]).astype(BF)

    def rope(u, gain_row, r):
        mean = jnp.mean(u * u, axis=-1, keepdims=True)
        u = u * lax.rsqrt(mean + EPSILON) * gain_row
        swapped = jnp.where(first_half, pltpu.roll(u, HEAD - 32, 1), pltpu.roll(u, 32, 1))
        per = third // GRID_W

        def table(which):
            return jnp.concatenate(
                [col_table[which] + rows_tab[which, pl.ds(r * per + i, 1), :] for i in range(per)], axis=0
            )

        return (u * table(0) + swapped * table(1)).astype(BF)

    def project_keys(r):
        rows = pl.ds(r * third, third)
        p = dot(xn[rows, :], wkv[...])
        kall[0, rows, :] = rope(p[:, 0:128], gain_k[...], r)
        vall[0, pl.ds(0, HEAD), rows] = p[:, 128:256].T.astype(BF)

    def project_queries(r):
        rows = pl.ds(r * third, third)
        p = dot(xn[rows, :], wqg[...])
        scaled = gain_q[...] * SCORE
        qr[0, rows, :] = rope(p[:, 0:128], scaled, r)
        qr[1, rows, :] = rope(p[:, 128:256], scaled, r)

    loads[0].wait()
    loads[3].start()
    norm(0)
    for i in (1, 2, 4, 5):
        loads[i].wait()
    for i in (7, 8, 9, 10, 11):
        loads[i].start()
    norm(1)
    project_keys(0)
    loads[6].wait()
    norm(2)
    project_keys(1)
    project_keys(2)

    pl.semaphore_wait(barrier, len(peers))
    value_rows = pl.ds(0, HEAD)
    sends = []

    def send(*args):
        copy = remote(*args)
        copy.start()
        sends.append(copy)

    def k_copy(slot_from, slot_to, s, d):
        return (kall.at[slot_from], kall.at[slot_to], kv_s.at[s], kv_r.at[0, slot_to], kv_peer(d))

    def v_copy(slot_from, slot_to, s, d):
        return (
            vall.at[slot_from, value_rows],
            vall.at[slot_to, value_rows],
            kv_s.at[s],
            kv_r.at[1, slot_to],
            kv_peer(d),
        )

    k_up, k_down = k_copy(0, 3, 0, 1), k_copy(0, 1, 1, 3)
    v_up, v_down = v_copy(0, 3, 2, 1), v_copy(0, 1, 3, 3)
    for args in (k_up, v_down, k_down, v_up):
        send(*args)
    k_relay, v_relay = k_copy(3, 2, 4, 1), v_copy(1, 2, 5, 3)

    loads[3].wait()
    for r in range(3):
        project_queries(r)
    ahead, behind, across = (lax.rem(x + d, SIDE) * 192 for d in (1, 3, 2))
    own = x * 192
    starts = (
        (across, across + 48, across + 96, across + 144),
        (ahead, behind, ahead + 96, behind + 96),
        (ahead + 48, behind + 48, ahead + 144, behind + 144),
        (own, own + 48, own + 96, own + 144),
    )

    def gather(ref, k):
        return jnp.concatenate([ref[pl.ds(pl.multiple_of(s, 16), PART), :] for s in starts[k]], axis=0)

    for k in range(BLOCKS):
        one, two = gather(qr.at[0], k), gather(qr.at[1], k)
        pieces = (one[:128], jnp.concatenate([one[128:], two[:64]], axis=0), two[64:])
        for i, piece in enumerate(pieces):
            turned = piece.astype(F32).T.astype(BF)
            qs[k, i] = turned
            qp[k * 10 + 9 if i == 2 else EARLY + 2 * k + i] = turned

    place = {2: 0, 1: 3, 3: 6}

    def q_copy(source, k, slot, s, d):
        return (source, qp.at[pl.ds(k * 10 + place[slot], 3)], q_s.at[k, s], q_r.at[k, slot], q_peer(d))

    def send_queries(k):
        send(*q_copy(qs.at[k], k, 3, 0, 1))
        send(*q_copy(qs.at[k], k, 1, 1, 3))

    def relay_queries(k):
        arrived = 3 if k % 2 == 0 else 1
        wait_queries(k, arrived)
        send(*q_copy(qp.at[pl.ds(k * 10 + place[arrived], 3)], k, 2, 2, 4 - arrived))

    def wait_queries(k, slot):
        args = q_copy(qs.at[k], k, slot, 0, 1)
        remote(*args).wait_recv()

    for k in (0, 1):
        send_queries(k)

    for i in (7, 8, 9):
        loads[i].wait()
    for r in range(3):
        rows = pl.ds(r * third, third)
        p = dot(xn[rows, :], wl[...])
        lq[rows, :] = (p[:, 0:256] * SCORE).astype(BF)
        lk[pl.ds(WINDOW + r * third, third), :] = p[:, 256:384].astype(BF)
        lv[pl.ds(WINDOW + r * third, third), :] = p[:, 384:512].astype(BF)

    def halo(ref, i, low):
        source, target, d = (ROWS, 0, 1) if low else (WINDOW, ROWS + WINDOW, NSP - 1)
        j = 2 * i + (0 if low else 1)
        return (
            ref.at[pl.ds(source, WINDOW)],
            ref.at[pl.ds(target, WINDOW)],
            h_s.at[j],
            h_r.at[j],
            sp_peer(d),
        )

    halos = [halo(ref, i, low) for i, ref in enumerate((lk, lv)) for low in (True, False)]
    for args in halos:
        send(*args)

    def attend(base, tiles, slots, count, tops=None, following=None):
        units = tiles * count // 2

        def where(u):
            halves = []
            for h in range(2):
                index = 2 * u + h
                halves.append((slots(index // tiles), base + lax.rem(index, tiles)))
            return halves

        def scores(halves, ref):
            tops = []
            for h, (t, g) in enumerate(halves):
                queries = jnp.concatenate([qp[2 * g], qp[2 * g + 1]], axis=1)
                s = dot(kall[t], queries)
                ref[h] = s
                tops.append(jnp.max(s, axis=0, keepdims=True))
            return tops

        def weigh(halves, ref, tops):
            for h, (t, g) in enumerate(halves):
                before = m[g]
                top = jnp.maximum(before, tops[h])
                factor = jnp.exp2(before - top)
                weights = jnp.exp2(ref[h] - top).astype(BF)
                result = dot(vall[t], weights)
                m[g] = top
                l[g] = l[g] * factor + result[HEAD : HEAD + 1]
                o[g] = o[g] * factor + result[:HEAD]

        if tops is None:
            tops = scores(where(0), s0)

        def body(i, tops):
            u = 2 * i
            later = scores(where(u + 1), s1)
            weigh(where(u), s0, tops)
            after = where(jnp.minimum(u + 2, units - 1))
            if following is not None:
                last = (i + 1) // (units // 2)
                after = [
                    (t * (1 - last) + ft * last, g * (1 - last) + fg * last)
                    for (t, g), (ft, fg) in zip(after, following)
                ]
            tops = scores(after, s0)
            weigh(where(u + 1), s1, later)
            return tops

        return lax.fori_loop(0, units // 2, body, tops)

    attend(EARLY // 2, 4, lambda i: i * 0, 1)

    wide = 3 * WINDOW
    row = lax.rem(lax.broadcasted_iota(jnp.int32, (2 * WINDOW, wide), 0), WINDOW)
    col = lax.broadcasted_iota(jnp.int32, (2 * WINDOW, wide), 1)
    near = (col >= row) & (col <= row + 2 * WINDOW)
    sink_rows = jnp.concatenate(
        [jnp.full((WINDOW, 1), sink[0] * LOG2E, F32), jnp.full((WINDOW, 1), sink[1] * LOG2E, F32)], axis=0
    )
    blocks = ROWS // WINDOW

    def banded(n, carry):
        at = pl.multiple_of(n * WINDOW, WINDOW)
        rows = lq[pl.ds(at, WINDOW), :]
        queries = jnp.concatenate([rows[:, :HEAD], rows[:, HEAD:]], axis=0)
        keys = lk[pl.ds(at, wide), :]
        s = lax.dot_general(queries, keys, (((1,), (1,)), ((), ())), preferred_element_type=F32)
        block = sp * blocks + n
        low = jnp.where(block == 0, WINDOW, 0)
        high = jnp.where(block == NSP * blocks - 1, 2 * WINDOW, wide)
        s = jnp.where(near & (col >= low) & (col < high), s, -1e30)
        top = jnp.maximum(jnp.max(s, axis=1, keepdims=True), sink_rows)
        lifted = jnp.exp2(s - top)
        total = jnp.sum(lifted, axis=1, keepdims=True) + jnp.exp2(sink_rows - top)
        result = dot(lifted.astype(BF), lv[pl.ds(at, wide), :]) / total
        lo[pl.ds(at, WINDOW), :] = jnp.concatenate([result[:WINDOW], result[WINDOW:]], axis=1).astype(BF)
        return carry

    lax.fori_loop(1, blocks - 1, banded, 0)

    remote(*k_up).wait_recv()
    send(*k_relay)
    remote(*v_down).wait_recv()
    send(*v_relay)
    relay_queries(0)
    relay_queries(1)
    for k in (2, 3):
        send_queries(k)
    remote(*k_down).wait_recv()
    remote(*v_up).wait_recv()
    attend(EARLY // 2, 4, lambda i: 1 + 2 * i, 2)
    for args in halos:
        remote(*args).wait_recv()
    lax.fori_loop(0, 2, lambda i, carry: banded(i * (blocks - 1), carry), 0)
    remote(*k_relay).wait_recv()
    remote(*v_relay).wait_recv()
    attend(EARLY // 2, 4, lambda i: i * 0 + 2, 1)

    def state(g):
        lanes = pl.ds(g % 2 * HEAD, HEAD)
        return m[g // 2, :, lanes], l[g // 2, :, lanes], o[g // 2, :, lanes]

    def packed(g):
        top, total, result = state(g)
        level = top + jnp.log2(total)
        high = level.astype(BF)
        rest = level - high.astype(F32)
        mid = rest.astype(BF)
        low = (rest - mid.astype(F32)).astype(BF)
        tail = jnp.concatenate([high, mid, low, jnp.zeros((13, HEAD), BF)], axis=0)
        return jnp.concatenate([(result * (1.0 / total)).astype(BF), tail], axis=0)

    def o_copy(k, s):
        return (osend.at[k, s], orecv.at[k, 4 - s], o_s.at[k, s], o_r.at[k, 4 - s], q_peer(s))

    def send_results(k, *targets):
        for s in targets:
            for i in range(3):
                osend[k, s, i] = packed(k * 10 + place[s] + i)
            send(*o_copy(k, s))

    def merge(k):
        for s in (1, 3, 2):
            remote(*o_copy(k, s)).wait_recv()
        merged = []
        for i in range(3):
            g = k * 10 + 9 if i == 2 else EARLY + 2 * k + i
            levels = []
            for s in (1, 2, 3):
                rows = orecv[k, s, i, pl.ds(HEAD, 16), :].astype(F32)
                levels.append(rows[0:1] + rows[1:2] + rows[2:3])
            highest, total, result = state(g)
            mine = highest + jnp.log2(total)
            top = functools.reduce(jnp.maximum, levels, mine)
            share = jnp.exp2(mine - top)
            shares = [jnp.exp2(level - top) for level in levels]
            whole = share + shares[0] + shares[1] + shares[2]
            acc = result * (share / (total * whole))
            for s in (1, 2, 3):
                acc += orecv[k, s, i, value_rows, :].astype(F32) * (shares[s - 1] / whole)
            merged.append(acc.T.astype(BF))
        one = jnp.concatenate([merged[0], merged[1][:64]], axis=0)
        two = jnp.concatenate([merged[1][64:], merged[2]], axis=0)
        features = jnp.concatenate([one, two, gather(lo, k)], axis=1)
        keep[k] = dot(features, wo[...])
        dsend[k] = keep[k, pl.ds(pl.multiple_of((1 - core) * 96, 16), 96), :].astype(BF)
        send(*d_copy(k))

    def d_copy(k):
        return (dsend.at[k], drecv.at[k], d_s.at[k], d_r.at[k], partner)

    half = D // 2

    def x_copy(i):
        if i < 2:
            return (x0.at[i], ra.at[i], x_s.at[i], x_r.at[i], x_peer(1 if i == 0 else 3))
        k, side = divmod(i - 2, 2)
        return (x12.at[k, side], r1.at[k, side], x_s.at[i], x_r.at[i], x_peer(1 if side == 0 else 3))

    def summed(k):
        remote(*d_copy(k)).wait_recv()
        return keep[k, pl.ds(pl.multiple_of(core * 96, 16), 96), :] + drecv[k].astype(F32)

    def scatter(k):
        total = summed(k)
        if k == 0:
            for i in range(2):
                x0[i] = total[:, i * half : i * half + half].astype(BF)
                send(*x_copy(i))
        elif k < 3:
            if k == 1:
                for i in range(2):
                    remote(*x_copy(i)).wait_recv()
            for side in range(2):
                mine = total[side * PART : side * PART + PART]
                passing = ra[side, pl.ds((k - 1) * PART, PART), :].astype(F32)
                if side == 0:
                    mine = jnp.concatenate([mine[:, :half] + passing, mine[:, half:]], axis=1)
                else:
                    mine = jnp.concatenate([mine[:, :half], mine[:, half:] + passing], axis=1)
                x12[k - 1, side] = mine.astype(BF)
                send(*x_copy(2 * k + side))
        else:
            for i in range(2, 6):
                remote(*x_copy(i)).wait_recv()
            for part in range(2):
                rows = slice(part * PART, part * PART + PART)
                both = r1[part, 0].astype(F32) + r1[part, 1].astype(F32)
                out[pl.ds(part * PART, PART), :] = (total[rows] + both).astype(BF)

    for i in (10, 11):
        loads[i].wait()
    def wait_block(k):
        wait_queries(k, 1 if k % 2 == 0 else 3)
        wait_queries(k, 2)

    wait_block(0)
    relay_queries(2)
    relay_queries(3)
    tops = None
    for k in range(BLOCKS):
        tops = attend(k * 5, 3, lambda i: i, SIDE, tops, [(0, k * 5 + 3), (0, k * 5 + 4)])
        send_results(k, 2, 1)
        if k > 1:
            scatter(k - 2)
        if k == BLOCKS - 1:
            merge(k - 1)
        following = None
        if k + 1 < BLOCKS:
            wait_block(k + 1)
            following = [(0, k * 5 + 5), (0, k * 5 + 6)]
        tops = attend(k * 5 + 3, 2, lambda i: i, SIDE, tops, following)
        send_results(k, 3)
        if k == BLOCKS - 1:
            scatter(k - 1)
        elif k > 0:
            merge(k - 1)
    merge(3)
    scatter(3)
    for copy in sends:
        copy.wait_send()


def shards(
    tokens,
    norm_gain,
    grid_query_weight,
    grid_key_weight,
    grid_value_weight,
    grid_query_gain,
    grid_key_gain,
    local_query_weight,
    local_key_weight,
    local_value_weight,
    sink_logit,
    grid_out_weight,
    local_out_weight,
):
    row_table, col_table = rope_tables()
    hbm = pl.BlockSpec(memory_space=pl.ANY)
    vmem = pl.BlockSpec(memory_space=pltpu.VMEM)
    smem = pl.BlockSpec(memory_space=pltpu.SMEM)
    dma = pltpu.SemaphoreType.DMA
    return pl.pallas_call(
        kernel,
        out_shape=jax.ShapeDtypeStruct((96, D), BF),
        in_specs=[hbm, vmem, hbm, hbm, hbm, vmem, vmem, hbm, hbm, hbm, smem, hbm, hbm, hbm, vmem],
        out_specs=vmem,
        scratch_shapes=[
            pltpu.VMEM((ROWS, D), BF),
            pltpu.VMEM((ROWS, D), BF),
            pltpu.VMEM((D, 256), BF),
            pltpu.VMEM((D, 256), BF),
            pltpu.VMEM((D, 512), BF),
            pltpu.VMEM((512, D), BF),
            pltpu.VMEM((2, 16, HEAD), F32),
            pltpu.VMEM((2, ROWS, HEAD), BF),
            pltpu.VMEM((BLOCKS, 3, HEAD, HEAD), BF),
            pltpu.VMEM((48, HEAD, HEAD), BF),
            pltpu.VMEM((SIDE, ROWS, HEAD), BF),
            pltpu.VMEM((SIDE, HEAD + 16, ROWS), BF),
            pltpu.VMEM((24, 1, 2 * HEAD), F32),
            pltpu.VMEM((24, 1, 2 * HEAD), F32),
            pltpu.VMEM((24, HEAD, 2 * HEAD), F32),
            pltpu.VMEM((2, ROWS, 256), F32),
            pltpu.VMEM((2, ROWS, 256), F32),
            pltpu.VMEM((ROWS, 256), BF),
            pltpu.VMEM((ROWS + 2 * WINDOW, HEAD), BF),
            pltpu.VMEM((ROWS + 2 * WINDOW, HEAD), BF),
            pltpu.VMEM((ROWS, 256), BF),
            pltpu.VMEM((BLOCKS, 4, 3, HEAD + 16, HEAD), BF),
            pltpu.VMEM((BLOCKS, 4, 3, HEAD + 16, HEAD), BF),
            pltpu.VMEM((BLOCKS, 192, D), F32),
            pltpu.VMEM((BLOCKS, 96, D), BF),
            pltpu.VMEM((BLOCKS, 96, D), BF),
            pltpu.VMEM((2, 96, D // 2), BF),
            pltpu.VMEM((2, 2, PART, D), BF),
            pltpu.VMEM((2, 96, D // 2), BF),
            pltpu.VMEM((2, 2, PART, D), BF),
            dma((12,)),
            dma((6,)),
            dma((2, 4)),
            dma((BLOCKS, 3)),
            dma((BLOCKS, 4)),
            dma((4,)),
            dma((4,)),
            dma((BLOCKS, 4)),
            dma((BLOCKS, 4)),
            dma((BLOCKS,)),
            dma((BLOCKS,)),
            dma((6,)),
            dma((6,)),
        ],
        compiler_params=pltpu.CompilerParams(
            collective_id=0, has_side_effects=True, vmem_limit_bytes=60 * 2**20
        ),
    )(
        tokens,
        norm_gain.reshape(1, D),
        grid_query_weight,
        grid_key_weight,
        grid_value_weight,
        grid_query_gain.reshape(1, HEAD),
        grid_key_gain.reshape(1, HEAD),
        local_query_weight,
        local_key_weight,
        local_value_weight,
        sink_logit,
        grid_out_weight,
        local_out_weight,
        jnp.asarray(row_table),
        jnp.asarray(col_table),
    )


def solution(mesh):
    in_specs = (
        P("sp", None),
        P(),
        P(None, "tp"),
        P(None, "tp"),
        P(None, "tp"),
        P(),
        P(),
        P(None, "tp"),
        P(None, "tp"),
        P(None, "tp"),
        P("tp"),
        P("tp", None),
        P("tp", None),
    )
    out_specs = P(("sp", "tp"), None)
    return jax.shard_map(shards, mesh=mesh, in_specs=in_specs, out_specs=out_specs, check_vma=False)
```

```python
import functools
import math

import jax
import jax.numpy as jnp
import numpy as np
from jax import lax
from jax.experimental import pallas as pl
from jax.experimental.pallas import tpu as pltpu
from jax.sharding import PartitionSpec as P

D = 2048
HEAD = 128
WINDOW = 128
GRID_W = 64
ROWS = 768
EPSILON = 1e-06
ROPE_BASE = 10000.0
LOG2E = math.log2(math.e)
SCORE = HEAD ** (-0.5) * LOG2E
NSP = 16
SIDE = 4
BLOCKS = 4
CHUNK = 32
PART = 48
EARLY = 40
BF = jnp.bfloat16
F32 = jnp.float32
MESH = pl.DeviceIdType.MESH


def dot(a, b):
    return jnp.dot(a, b, preferred_element_type=F32)


def rope_tables():
    half = HEAD // 2
    inverse = ROPE_BASE ** (-np.arange(0, half, 2, dtype=np.float64) / half)
    sign = np.concatenate([-np.ones(half // 2), np.ones(half // 2)])

    def table(count):
        angle = np.arange(count)[:, None] * np.concatenate([inverse, inverse])
        return np.cos(angle), np.sin(angle) * sign

    rows = np.zeros((2, NSP, 16, HEAD), np.float32)
    cosine, sine = table(NSP * ROWS // GRID_W)
    per = ROWS // GRID_W
    rows[0, :, :per, :half] = cosine.reshape(NSP, per, half)
    rows[1, :, :per, :half] = sine.reshape(NSP, per, half)
    cols = np.zeros((2, GRID_W, HEAD), np.float32)
    cosine, sine = table(GRID_W)
    cols[0, :, half:] = cosine
    cols[1, :, half:] = sine
    return np.ascontiguousarray(rows.transpose(1, 0, 2, 3)), cols


def kernel(
    tokens,
    gain,
    wq,
    wk,
    wv,
    gain_q,
    gain_k,
    lwq,
    lwk,
    lwv,
    sink,
    wog,
    wol,
    row_table,
    col_table,
    out,
    xs,
    xn,
    wkv,
    wqg,
    wl,
    wo,
    rows_tab,
    qr,
    qs,
    qp,
    kall,
    vall,
    m,
    l,
    o,
    s0,
    s1,
    lq,
    lk,
    lv,
    lo,
    osend,
    orecv,
    keep,
    dsend,
    drecv,
    x0,
    x12,
    ra,
    r1,
    in_sem,
    kv_s,
    kv_r,
    q_s,
    q_r,
    h_s,
    h_r,
    o_s,
    o_r,
    d_s,
    d_r,
    x_s,
    x_r,
):
    sp = lax.axis_index("sp")
    tp = lax.axis_index("tp")
    core = lax.rem(tp, 2)
    x = tp // 2
    z = sp // SIDE
    y = lax.rem(sp, SIDE)

    def along_z(d):
        return lax.rem(z + d, SIDE) * SIDE + y

    def along_y(d):
        return z * SIDE + lax.rem(y + d, SIDE)

    def q_peer(d):
        return {"sp": along_z(d) * (1 - core) + along_y(d) * core, "tp": tp}

    def kv_peer(d):
        return {"sp": along_z(d) * core + along_y(d) * (1 - core), "tp": tp}

    def sp_peer(d):
        return {"sp": lax.rem(sp + d, NSP), "tp": tp}

    def x_peer(d):
        return {"sp": sp, "tp": lax.rem(x + d, SIDE) * 2 + core}

    partner = {"sp": sp, "tp": x * 2 + 1 - core}

    def remote(src, dst, send, recv, peer):
        return pltpu.make_async_remote_copy(
            src_ref=src, dst_ref=dst, send_sem=send, recv_sem=recv, device_id=peer, device_id_type=MESH
        )

    def local(src, dst, i):
        return pltpu.make_async_copy(src, dst, in_sem.at[i])

    third = ROWS // 3
    loads = [
        local(tokens.at[pl.ds(0, third)], xs.at[pl.ds(0, third)], 0),
        local(wk, wkv.at[:, pl.ds(0, 128)], 1),
        local(wv, wkv.at[:, pl.ds(128, 128)], 2),
        local(row_table.at[sp], rows_tab, 4),
        local(tokens.at[pl.ds(third, third)], xs.at[pl.ds(third, third)], 5),
        local(tokens.at[pl.ds(2 * third, third)], xs.at[pl.ds(2 * third, third)], 6),
        local(wq, wqg, 3),
        local(lwq, wl.at[:, pl.ds(0, 256)], 7),
        local(lwk, wl.at[:, pl.ds(256, 128)], 8),
        local(lwv, wl.at[:, pl.ds(384, 128)], 9),
        local(wog, wo.at[pl.ds(0, 256)], 10),
        local(wol, wo.at[pl.ds(256, 256)], 11),
    ]
    loads = dict(zip((0, 1, 2, 4, 5, 6, 3, 7, 8, 9, 10, 11), loads))
    for i in (0, 1, 2, 4, 5, 6):
        loads[i].start()

    barrier = pltpu.get_barrier_semaphore()
    peers = [q_peer(1), q_peer(2), q_peer(3), kv_peer(1), kv_peer(3), sp_peer(1), sp_peer(NSP - 1)]
    peers += [x_peer(1), x_peer(3), partner]
    for peer in peers:
        pl.semaphore_signal(barrier, inc=1, device_id=peer, device_id_type=MESH)

    m[...] = jnp.full_like(m, -1e30)
    l[...] = jnp.zeros_like(l)
    o[...] = jnp.zeros_like(o)
    vall[:, pl.ds(HEAD, 16), :] = jnp.ones((SIDE, 16, ROWS), BF)

    lane = lax.broadcasted_iota(jnp.int32, (third, HEAD), 1)
    first_half = lax.rem(lane, 64) < 32

    def norm(r):
        for c in range(third // CHUNK):
            rows = pl.ds(r * third + c * CHUNK, CHUNK)
            squares = jnp.zeros((CHUNK, HEAD), F32)
            for j in range(D // HEAD):
                part = xs[rows, pl.ds(j * HEAD, HEAD)].astype(F32)
                squares += part * part
            factor = lax.rsqrt(jnp.sum(squares, axis=-1, keepdims=True) / D + EPSILON)
            for j in range(D // HEAD):
                cols = pl.ds(j * HEAD, HEAD)
                xn[rows, cols] = (xs[rows, cols].astype(F32) * factor * gain[:, cols]).astype(BF)

    def rope(u, gain_row, r):
        mean = jnp.mean(u * u, axis=-1, keepdims=True)
        u = u * lax.rsqrt(mean + EPSILON) * gain_row
        swapped = jnp.where(first_half, pltpu.roll(u, HEAD - 32, 1), pltpu.roll(u, 32, 1))
        per = third // GRID_W

        def table(which):
            return jnp.concatenate(
                [col_table[which] + rows_tab[which, pl.ds(r * per + i, 1), :] for i in range(per)], axis=0
            )

        return (u * table(0) + swapped * table(1)).astype(BF)

    def project_keys(r):
        rows = pl.ds(r * third, third)
        p = dot(xn[rows, :], wkv[...])
        kall[0, rows, :] = rope(p[:, 0:128], gain_k[...], r)
        vall[0, pl.ds(0, HEAD), rows] = p[:, 128:256].T.astype(BF)

    def project_queries(r):
        rows = pl.ds(r * third, third)
        p = dot(xn[rows, :], wqg[...])
        scaled = gain_q[...] * SCORE
        qr[0, rows, :] = rope(p[:, 0:128], scaled, r)
        qr[1, rows, :] = rope(p[:, 128:256], scaled, r)

    loads[0].wait()
    loads[3].start()
    norm(0)
    for i in (1, 2, 4, 5):
        loads[i].wait()
    for i in (7, 8, 9, 10, 11):
        loads[i].start()
    norm(1)
    project_keys(0)
    loads[6].wait()
    norm(2)
    project_keys(1)
    project_keys(2)

    pl.semaphore_wait(barrier, len(peers))
    value_rows = pl.ds(0, HEAD)
    sends = []

    def send(*args):
        copy = remote(*args)
        copy.start()
        sends.append(copy)

    def k_copy(slot_from, slot_to, s, d):
        return (kall.at[slot_from], kall.at[slot_to], kv_s.at[s], kv_r.at[0, slot_to], kv_peer(d))

    def v_copy(slot_from, slot_to, s, d):
        return (
            vall.at[slot_from, value_rows],
            vall.at[slot_to, value_rows],
            kv_s.at[s],
            kv_r.at[1, slot_to],
            kv_peer(d),
        )

    k_up, k_down = k_copy(0, 3, 0, 1), k_copy(0, 1, 1, 3)
    v_up, v_down = v_copy(0, 3, 2, 1), v_copy(0, 1, 3, 3)
    for args in (k_up, v_down, k_down, v_up):
        send(*args)
    k_relay, v_relay = k_copy(3, 2, 4, 1), v_copy(1, 2, 5, 3)

    loads[3].wait()
    for r in range(3):
        project_queries(r)
    ahead, behind, across = (lax.rem(x + d, SIDE) * 192 for d in (1, 3, 2))
    own = x * 192
    starts = (
        (across, across + 48, across + 96, across + 144),
        (ahead, behind, ahead + 96, behind + 96),
        (ahead + 48, behind + 48, ahead + 144, behind + 144),
        (own, own + 48, own + 96, own + 144),
    )

    def gather(ref, k):
        return jnp.concatenate([ref[pl.ds(pl.multiple_of(s, 16), PART), :] for s in starts[k]], axis=0)

    for k in range(BLOCKS):
        one, two = gather(qr.at[0], k), gather(qr.at[1], k)
        pieces = (one[:128], jnp.concatenate([one[128:], two[:64]], axis=0), two[64:])
        for i, piece in enumerate(pieces):
            turned = piece.astype(F32).T.astype(BF)
            qs[k, i] = turned
            qp[k * 10 + 9 if i == 2 else EARLY + 2 * k + i] = turned

    place = {2: 0, 1: 3, 3: 6}

    def q_copy(source, k, slot, s, d):
        return (source, qp.at[pl.ds(k * 10 + place[slot], 3)], q_s.at[k, s], q_r.at[k, slot], q_peer(d))

    def send_queries(k):
        send(*q_copy(qs.at[k], k, 3, 0, 1))
        send(*q_copy(qs.at[k], k, 1, 1, 3))

    def relay_queries(k):
        arrived = 3 if k % 2 == 0 else 1
        wait_queries(k, arrived)
        send(*q_copy(qp.at[pl.ds(k * 10 + place[arrived], 3)], k, 2, 2, 4 - arrived))

    def wait_queries(k, slot):
        args = q_copy(qs.at[k], k, slot, 0, 1)
        remote(*args).wait_recv()

    send_queries(0)

    for i in (7, 8, 9):
        loads[i].wait()
    for r in range(3):
        rows = pl.ds(r * third, third)
        p = dot(xn[rows, :], wl[...])
        lq[rows, :] = (p[:, 0:256] * SCORE).astype(BF)
        lk[pl.ds(WINDOW + r * third, third), :] = p[:, 256:384].astype(BF)
        lv[pl.ds(WINDOW + r * third, third), :] = p[:, 384:512].astype(BF)

    def halo(ref, i, low):
        source, target, d = (ROWS, 0, 1) if low else (WINDOW, ROWS + WINDOW, NSP - 1)
        j = 2 * i + (0 if low else 1)
        return (
            ref.at[pl.ds(source, WINDOW)],
            ref.at[pl.ds(target, WINDOW)],
            h_s.at[j],
            h_r.at[j],
            sp_peer(d),
        )

    halos = [halo(ref, i, low) for i, ref in enumerate((lk, lv)) for low in (True, False)]
    for args in halos:
        send(*args)

    def attend(base, tiles, slots, count, tops=None, following=None):
        units = tiles * count // 2

        def where(u):
            halves = []
            for h in range(2):
                index = 2 * u + h
                halves.append((slots(index // tiles), base + lax.rem(index, tiles)))
            return halves

        def scores(halves, ref):
            tops = []
            for h, (t, g) in enumerate(halves):
                queries = jnp.concatenate([qp[2 * g], qp[2 * g + 1]], axis=1)
                s = dot(kall[t], queries)
                ref[h] = s
                tops.append(jnp.max(s, axis=0, keepdims=True))
            return tops

        def weigh(halves, ref, tops):
            for h, (t, g) in enumerate(halves):
                before = m[g]
                top = jnp.maximum(before, tops[h])
                factor = jnp.exp2(before - top)
                weights = jnp.exp2(ref[h] - top).astype(BF)
                result = dot(vall[t], weights)
                m[g] = top
                l[g] = l[g] * factor + result[HEAD : HEAD + 1]
                o[g] = o[g] * factor + result[:HEAD]

        if tops is None:
            tops = scores(where(0), s0)

        def body(i, tops):
            u = 2 * i
            later = scores(where(u + 1), s1)
            weigh(where(u), s0, tops)
            after = where(jnp.minimum(u + 2, units - 1))
            if following is not None:
                last = (i + 1) // (units // 2)
                after = [
                    (t * (1 - last) + ft * last, g * (1 - last) + fg * last)
                    for (t, g), (ft, fg) in zip(after, following)
                ]
            tops = scores(after, s0)
            weigh(where(u + 1), s1, later)
            return tops

        return lax.fori_loop(0, units // 2, body, tops)

    attend(EARLY // 2, 4, lambda i: i * 0, 1)

    wide = 3 * WINDOW
    row = lax.rem(lax.broadcasted_iota(jnp.int32, (2 * WINDOW, wide), 0), WINDOW)
    col = lax.broadcasted_iota(jnp.int32, (2 * WINDOW, wide), 1)
    near = (col >= row) & (col <= row + 2 * WINDOW)
    sink_rows = jnp.concatenate(
        [jnp.full((WINDOW, 1), sink[0] * LOG2E, F32), jnp.full((WINDOW, 1), sink[1] * LOG2E, F32)], axis=0
    )
    blocks = ROWS // WINDOW

    def banded(n, carry):
        at = pl.multiple_of(n * WINDOW, WINDOW)
        rows = lq[pl.ds(at, WINDOW), :]
        queries = jnp.concatenate([rows[:, :HEAD], rows[:, HEAD:]], axis=0)
        keys = lk[pl.ds(at, wide), :]
        s = lax.dot_general(queries, keys, (((1,), (1,)), ((), ())), preferred_element_type=F32)
        block = sp * blocks + n
        low = jnp.where(block == 0, WINDOW, 0)
        high = jnp.where(block == NSP * blocks - 1, 2 * WINDOW, wide)
        s = jnp.where(near & (col >= low) & (col < high), s, -1e30)
        top = jnp.maximum(jnp.max(s, axis=1, keepdims=True), sink_rows)
        lifted = jnp.exp2(s - top)
        total = jnp.sum(lifted, axis=1, keepdims=True) + jnp.exp2(sink_rows - top)
        result = dot(lifted.astype(BF), lv[pl.ds(at, wide), :]) / total
        lo[pl.ds(at, WINDOW), :] = jnp.concatenate([result[:WINDOW], result[WINDOW:]], axis=1).astype(BF)
        return carry

    lax.fori_loop(1, blocks - 1, banded, 0)

    remote(*k_up).wait_recv()
    send(*k_relay)
    remote(*v_down).wait_recv()
    send(*v_relay)
    relay_queries(0)
    for k in (1, 2, 3):
        send_queries(k)
    remote(*k_down).wait_recv()
    remote(*v_up).wait_recv()
    attend(EARLY // 2, 4, lambda i: 1 + 2 * i, 2)
    for args in halos:
        remote(*args).wait_recv()
    lax.fori_loop(0, 2, lambda i, carry: banded(i * (blocks - 1), carry), 0)
    relay_queries(1)
    remote(*k_relay).wait_recv()
    remote(*v_relay).wait_recv()
    attend(EARLY // 2, 4, lambda i: i * 0 + 2, 1)

    def state(g):
        lanes = pl.ds(g % 2 * HEAD, HEAD)
        return m[g // 2, :, lanes], l[g // 2, :, lanes], o[g // 2, :, lanes]

    def packed(g):
        top, total, result = state(g)
        level = top + jnp.log2(total)
        high = level.astype(BF)
        rest = level - high.astype(F32)
        mid = rest.astype(BF)
        low = (rest - mid.astype(F32)).astype(BF)
        tail = jnp.concatenate([high, mid, low, jnp.zeros((13, HEAD), BF)], axis=0)
        return jnp.concatenate([(result * (1.0 / total)).astype(BF), tail], axis=0)

    def o_copy(k, s):
        return (osend.at[k, s], orecv.at[k, 4 - s], o_s.at[k, s], o_r.at[k, 4 - s], q_peer(s))

    def send_results(k, *targets):
        for s in targets:
            for i in range(3):
                osend[k, s, i] = packed(k * 10 + place[s] + i)
            send(*o_copy(k, s))

    def merge(k):
        for s in (1, 3, 2):
            remote(*o_copy(k, s)).wait_recv()
        merged = []
        for i in range(3):
            g = k * 10 + 9 if i == 2 else EARLY + 2 * k + i
            levels = []
            for s in (1, 2, 3):
                rows = orecv[k, s, i, pl.ds(HEAD, 16), :].astype(F32)
                levels.append(rows[0:1] + rows[1:2] + rows[2:3])
            highest, total, result = state(g)
            mine = highest + jnp.log2(total)
            top = functools.reduce(jnp.maximum, levels, mine)
            share = jnp.exp2(mine - top)
            shares = [jnp.exp2(level - top) for level in levels]
            whole = share + shares[0] + shares[1] + shares[2]
            acc = result * (share / (total * whole))
            for s in (1, 2, 3):
                acc += orecv[k, s, i, value_rows, :].astype(F32) * (shares[s - 1] / whole)
            merged.append(acc.T.astype(BF))
        one = jnp.concatenate([merged[0], merged[1][:64]], axis=0)
        two = jnp.concatenate([merged[1][64:], merged[2]], axis=0)
        features = jnp.concatenate([one, two, gather(lo, k)], axis=1)
        keep[k] = dot(features, wo[...])
        dsend[k] = keep[k, pl.ds(pl.multiple_of((1 - core) * 96, 16), 96), :].astype(BF)
        send(*d_copy(k))

    def d_copy(k):
        return (dsend.at[k], drecv.at[k], d_s.at[k], d_r.at[k], partner)

    half = D // 2

    def x_copy(i):
        if i < 2:
            return (x0.at[i], ra.at[i], x_s.at[i], x_r.at[i], x_peer(1 if i == 0 else 3))
        k, side = divmod(i - 2, 2)
        return (x12.at[k, side], r1.at[k, side], x_s.at[i], x_r.at[i], x_peer(1 if side == 0 else 3))

    def summed(k):
        remote(*d_copy(k)).wait_recv()
        return keep[k, pl.ds(pl.multiple_of(core * 96, 16), 96), :] + drecv[k].astype(F32)

    def scatter(k):
        total = summed(k)
        if k == 0:
            for i in range(2):
                x0[i] = total[:, i * half : i * half + half].astype(BF)
                send(*x_copy(i))
        elif k < 3:
            if k == 1:
                for i in range(2):
                    remote(*x_copy(i)).wait_recv()
            for side in range(2):
                mine = total[side * PART : side * PART + PART]
                passing = ra[side, pl.ds((k - 1) * PART, PART), :].astype(F32)
                if side == 0:
                    mine = jnp.concatenate([mine[:, :half] + passing, mine[:, half:]], axis=1)
                else:
                    mine = jnp.concatenate([mine[:, :half], mine[:, half:] + passing], axis=1)
                x12[k - 1, side] = mine.astype(BF)
                send(*x_copy(2 * k + side))
        else:
            for i in range(2, 6):
                remote(*x_copy(i)).wait_recv()
            for part in range(2):
                rows = slice(part * PART, part * PART + PART)
                both = r1[part, 0].astype(F32) + r1[part, 1].astype(F32)
                out[pl.ds(part * PART, PART), :] = (total[rows] + both).astype(BF)

    for i in (10, 11):
        loads[i].wait()
    def wait_block(k):
        wait_queries(k, 1 if k % 2 == 0 else 3)
        wait_queries(k, 2)

    wait_block(0)
    relay_queries(2)
    relay_queries(3)
    tops = None
    for k in range(BLOCKS):
        tops = attend(k * 5, 3, lambda i: i, SIDE, tops, [(0, k * 5 + 3), (0, k * 5 + 4)])
        send_results(k, 2, 1)
        if k > 1:
            scatter(k - 2)
        if k == BLOCKS - 1:
            merge(k - 1)
        following = None
        if k + 1 < BLOCKS:
            wait_block(k + 1)
            following = [(0, k * 5 + 5), (0, k * 5 + 6)]
        tops = attend(k * 5 + 3, 2, lambda i: i, SIDE, tops, following)
        send_results(k, 3)
        if k == BLOCKS - 1:
            scatter(k - 1)
        elif k > 0:
            merge(k - 1)
    merge(3)
    scatter(3)
    for copy in sends:
        copy.wait_send()


def shards(
    tokens,
    norm_gain,
    grid_query_weight,
    grid_key_weight,
    grid_value_weight,
    grid_query_gain,
    grid_key_gain,
    local_query_weight,
    local_key_weight,
    local_value_weight,
    sink_logit,
    grid_out_weight,
    local_out_weight,
):
    row_table, col_table = rope_tables()
    hbm = pl.BlockSpec(memory_space=pl.ANY)
    vmem = pl.BlockSpec(memory_space=pltpu.VMEM)
    smem = pl.BlockSpec(memory_space=pltpu.SMEM)
    dma = pltpu.SemaphoreType.DMA
    return pl.pallas_call(
        kernel,
        out_shape=jax.ShapeDtypeStruct((96, D), BF),
        in_specs=[hbm, vmem, hbm, hbm, hbm, vmem, vmem, hbm, hbm, hbm, smem, hbm, hbm, hbm, vmem],
        out_specs=vmem,
        scratch_shapes=[
            pltpu.VMEM((ROWS, D), BF),
            pltpu.VMEM((ROWS, D), BF),
            pltpu.VMEM((D, 256), BF),
            pltpu.VMEM((D, 256), BF),
            pltpu.VMEM((D, 512), BF),
            pltpu.VMEM((512, D), BF),
            pltpu.VMEM((2, 16, HEAD), F32),
            pltpu.VMEM((2, ROWS, HEAD), BF),
            pltpu.VMEM((BLOCKS, 3, HEAD, HEAD), BF),
            pltpu.VMEM((48, HEAD, HEAD), BF),
            pltpu.VMEM((SIDE, ROWS, HEAD), BF),
            pltpu.VMEM((SIDE, HEAD + 16, ROWS), BF),
            pltpu.VMEM((24, 1, 2 * HEAD), F32),
            pltpu.VMEM((24, 1, 2 * HEAD), F32),
            pltpu.VMEM((24, HEAD, 2 * HEAD), F32),
            pltpu.VMEM((2, ROWS, 256), F32),
            pltpu.VMEM((2, ROWS, 256), F32),
            pltpu.VMEM((ROWS, 256), BF),
            pltpu.VMEM((ROWS + 2 * WINDOW, HEAD), BF),
            pltpu.VMEM((ROWS + 2 * WINDOW, HEAD), BF),
            pltpu.VMEM((ROWS, 256), BF),
            pltpu.VMEM((BLOCKS, 4, 3, HEAD + 16, HEAD), BF),
            pltpu.VMEM((BLOCKS, 4, 3, HEAD + 16, HEAD), BF),
            pltpu.VMEM((BLOCKS, 192, D), F32),
            pltpu.VMEM((BLOCKS, 96, D), BF),
            pltpu.VMEM((BLOCKS, 96, D), BF),
            pltpu.VMEM((2, 96, D // 2), BF),
            pltpu.VMEM((2, 2, PART, D), BF),
            pltpu.VMEM((2, 96, D // 2), BF),
            pltpu.VMEM((2, 2, PART, D), BF),
            dma((12,)),
            dma((6,)),
            dma((2, 4)),
            dma((BLOCKS, 3)),
            dma((BLOCKS, 4)),
            dma((4,)),
            dma((4,)),
            dma((BLOCKS, 4)),
            dma((BLOCKS, 4)),
            dma((BLOCKS,)),
            dma((BLOCKS,)),
            dma((6,)),
            dma((6,)),
        ],
        compiler_params=pltpu.CompilerParams(
            collective_id=0, has_side_effects=True, vmem_limit_bytes=60 * 2**20
        ),
    )(
        tokens,
        norm_gain.reshape(1, D),
        grid_query_weight,
        grid_key_weight,
        grid_value_weight,
        grid_query_gain.reshape(1, HEAD),
        grid_key_gain.reshape(1, HEAD),
        local_query_weight,
        local_key_weight,
        local_value_weight,
        sink_logit,
        grid_out_weight,
        local_out_weight,
        jnp.asarray(row_table),
        jnp.asarray(col_table),
    )


def solution(mesh):
    in_specs = (
        P("sp", None),
        P(),
        P(None, "tp"),
        P(None, "tp"),
        P(None, "tp"),
        P(),
        P(),
        P(None, "tp"),
        P(None, "tp"),
        P(None, "tp"),
        P("tp"),
        P("tp", None),
        P("tp", None),
    )
    out_specs = P(("sp", "tp"), None)
    return jax.shard_map(shards, mesh=mesh, in_specs=in_specs, out_specs=out_specs, check_vma=False)
```

```python
import functools
import math

import jax
import jax.numpy as jnp
import numpy as np
from jax import lax
from jax.experimental import pallas as pl
from jax.experimental.pallas import tpu as pltpu
from jax.sharding import PartitionSpec as P

D = 2048
HEAD = 128
WINDOW = 128
GRID_W = 64
ROWS = 768
EPSILON = 1e-06
ROPE_BASE = 10000.0
LOG2E = math.log2(math.e)
SCORE = HEAD ** (-0.5) * LOG2E
NSP = 16
SIDE = 4
BLOCKS = 4
CHUNK = 32
PART = 48
EARLY = 40
BF = jnp.bfloat16
F32 = jnp.float32
MESH = pl.DeviceIdType.MESH


def dot(a, b):
    return jnp.dot(a, b, preferred_element_type=F32)


def rope_tables():
    half = HEAD // 2
    inverse = ROPE_BASE ** (-np.arange(0, half, 2, dtype=np.float64) / half)
    sign = np.concatenate([-np.ones(half // 2), np.ones(half // 2)])

    def table(count):
        angle = np.arange(count)[:, None] * np.concatenate([inverse, inverse])
        return np.cos(angle), np.sin(angle) * sign

    rows = np.zeros((2, NSP, 16, HEAD), np.float32)
    cosine, sine = table(NSP * ROWS // GRID_W)
    per = ROWS // GRID_W
    rows[0, :, :per, :half] = cosine.reshape(NSP, per, half)
    rows[1, :, :per, :half] = sine.reshape(NSP, per, half)
    cols = np.zeros((2, GRID_W, HEAD), np.float32)
    cosine, sine = table(GRID_W)
    cols[0, :, half:] = cosine
    cols[1, :, half:] = sine
    return np.ascontiguousarray(rows.transpose(1, 0, 2, 3)), cols


def kernel(
    tokens,
    gain,
    wq,
    wk,
    wv,
    gain_q,
    gain_k,
    lwq,
    lwk,
    lwv,
    sink,
    wog,
    wol,
    row_table,
    col_table,
    out,
    xs,
    xn,
    wkv,
    wqg,
    wl,
    wo,
    rows_tab,
    qr,
    qs,
    qp,
    kall,
    vall,
    m,
    l,
    o,
    s0,
    s1,
    lq,
    lk,
    lv,
    lo,
    osend,
    orecv,
    keep,
    dsend,
    drecv,
    x0,
    x12,
    ra,
    r1,
    in_sem,
    kv_s,
    kv_r,
    q_s,
    q_r,
    h_s,
    h_r,
    o_s,
    o_r,
    d_s,
    d_r,
    x_s,
    x_r,
):
    sp = lax.axis_index("sp")
    tp = lax.axis_index("tp")
    core = lax.rem(tp, 2)
    x = tp // 2
    z = sp // SIDE
    y = lax.rem(sp, SIDE)

    def along_z(d):
        return lax.rem(z + d, SIDE) * SIDE + y

    def along_y(d):
        return z * SIDE + lax.rem(y + d, SIDE)

    def q_peer(d):
        return {"sp": along_z(d) * (1 - core) + along_y(d) * core, "tp": tp}

    def kv_peer(d):
        return {"sp": along_z(d) * core + along_y(d) * (1 - core), "tp": tp}

    def sp_peer(d):
        return {"sp": lax.rem(sp + d, NSP), "tp": tp}

    def x_peer(d):
        return {"sp": sp, "tp": lax.rem(x + d, SIDE) * 2 + core}

    partner = {"sp": sp, "tp": x * 2 + 1 - core}

    def remote(src, dst, send, recv, peer):
        return pltpu.make_async_remote_copy(
            src_ref=src, dst_ref=dst, send_sem=send, recv_sem=recv, device_id=peer, device_id_type=MESH
        )

    def local(src, dst, i):
        return pltpu.make_async_copy(src, dst, in_sem.at[i])

    third = ROWS // 3
    loads = [
        local(tokens.at[pl.ds(0, third)], xs.at[pl.ds(0, third)], 0),
        local(wk, wkv.at[:, pl.ds(0, 128)], 1),
        local(wv, wkv.at[:, pl.ds(128, 128)], 2),
        local(row_table.at[sp], rows_tab, 4),
        local(tokens.at[pl.ds(third, third)], xs.at[pl.ds(third, third)], 5),
        local(tokens.at[pl.ds(2 * third, third)], xs.at[pl.ds(2 * third, third)], 6),
        local(wq, wqg, 3),
        local(lwq, wl.at[:, pl.ds(0, 256)], 7),
        local(lwk, wl.at[:, pl.ds(256, 128)], 8),
        local(lwv, wl.at[:, pl.ds(384, 128)], 9),
        local(wog, wo.at[pl.ds(0, 256)], 10),
        local(wol, wo.at[pl.ds(256, 256)], 11),
    ]
    loads = dict(zip((0, 1, 2, 4, 5, 6, 3, 7, 8, 9, 10, 11), loads))
    for i in (0, 1, 2, 4, 5, 6):
        loads[i].start()

    barrier = pltpu.get_barrier_semaphore()
    peers = [q_peer(1), q_peer(2), q_peer(3), kv_peer(1), kv_peer(3), sp_peer(1), sp_peer(NSP - 1)]
    peers += [x_peer(1), x_peer(3), partner]
    for peer in peers:
        pl.semaphore_signal(barrier, inc=1, device_id=peer, device_id_type=MESH)

    m[...] = jnp.full_like(m, -1e30)
    l[...] = jnp.zeros_like(l)
    o[...] = jnp.zeros_like(o)
    vall[:, pl.ds(HEAD, 16), :] = jnp.ones((SIDE, 16, ROWS), BF)

    lane = lax.broadcasted_iota(jnp.int32, (third, HEAD), 1)
    first_half = lax.rem(lane, 64) < 32

    def norm(r):
        for c in range(third // CHUNK):
            rows = pl.ds(r * third + c * CHUNK, CHUNK)
            squares = jnp.zeros((CHUNK, HEAD), F32)
            for j in range(D // HEAD):
                part = xs[rows, pl.ds(j * HEAD, HEAD)].astype(F32)
                squares += part * part
            factor = lax.rsqrt(jnp.sum(squares, axis=-1, keepdims=True) / D + EPSILON)
            for j in range(D // HEAD):
                cols = pl.ds(j * HEAD, HEAD)
                xn[rows, cols] = (xs[rows, cols].astype(F32) * factor * gain[:, cols]).astype(BF)

    def rope(u, gain_row, r):
        mean = jnp.mean(u * u, axis=-1, keepdims=True)
        u = u * lax.rsqrt(mean + EPSILON) * gain_row
        swapped = jnp.where(first_half, pltpu.roll(u, HEAD - 32, 1), pltpu.roll(u, 32, 1))
        per = third // GRID_W

        def table(which):
            return jnp.concatenate(
                [col_table[which] + rows_tab[which, pl.ds(r * per + i, 1), :] for i in range(per)], axis=0
            )

        return (u * table(0) + swapped * table(1)).astype(BF)

    def project_keys(r):
        rows = pl.ds(r * third, third)
        p = dot(xn[rows, :], wkv[...])
        kall[0, rows, :] = rope(p[:, 0:128], gain_k[...], r)
        vall[0, pl.ds(0, HEAD), rows] = p[:, 128:256].T.astype(BF)

    def project_queries(r):
        rows = pl.ds(r * third, third)
        p = dot(xn[rows, :], wqg[...])
        scaled = gain_q[...] * SCORE
        qr[0, rows, :] = rope(p[:, 0:128], scaled, r)
        qr[1, rows, :] = rope(p[:, 128:256], scaled, r)

    loads[0].wait()
    loads[3].start()
    norm(0)
    for i in (1, 2, 4, 5):
        loads[i].wait()
    for i in (7, 8, 9, 10, 11):
        loads[i].start()
    norm(1)
    project_keys(0)
    loads[6].wait()
    norm(2)
    project_keys(1)
    project_keys(2)

    pl.semaphore_wait(barrier, len(peers))
    value_rows = pl.ds(0, HEAD)
    sends = []

    def send(*args):
        copy = remote(*args)
        copy.start()
        sends.append(copy)

    def k_copy(slot_from, slot_to, s, d):
        return (kall.at[slot_from], kall.at[slot_to], kv_s.at[s], kv_r.at[0, slot_to], kv_peer(d))

    def v_copy(slot_from, slot_to, s, d):
        return (
            vall.at[slot_from, value_rows],
            vall.at[slot_to, value_rows],
            kv_s.at[s],
            kv_r.at[1, slot_to],
            kv_peer(d),
        )

    k_up, k_down = k_copy(0, 3, 0, 1), k_copy(0, 1, 1, 3)
    v_up, v_down = v_copy(0, 3, 2, 1), v_copy(0, 1, 3, 3)
    for args in (k_up, v_down, k_down, v_up):
        send(*args)
    k_relay, v_relay = k_copy(3, 2, 4, 1), v_copy(1, 2, 5, 3)

    loads[3].wait()
    for r in range(3):
        project_queries(r)
    ahead, behind, across = (lax.rem(x + d, SIDE) * 192 for d in (1, 3, 2))
    own = x * 192
    starts = (
        (across, across + 48, across + 96, across + 144),
        (ahead, behind, ahead + 96, behind + 96),
        (ahead + 48, behind + 48, ahead + 144, behind + 144),
        (own, own + 48, own + 96, own + 144),
    )

    def gather(ref, k):
        return jnp.concatenate([ref[pl.ds(pl.multiple_of(s, 16), PART), :] for s in starts[k]], axis=0)

    for k in range(BLOCKS):
        one, two = gather(qr.at[0], k), gather(qr.at[1], k)
        pieces = (one[:128], jnp.concatenate([one[128:], two[:64]], axis=0), two[64:])
        for i, piece in enumerate(pieces):
            turned = piece.astype(F32).T.astype(BF)
            qs[k, i] = turned
            qp[k * 10 + 9 if i == 2 else EARLY + 2 * k + i] = turned

    place = {2: 0, 1: 3, 3: 6}

    def q_copy(source, k, slot, s, d):
        return (source, qp.at[pl.ds(k * 10 + place[slot], 3)], q_s.at[k, s], q_r.at[k, slot], q_peer(d))

    def send_queries(k):
        send(*q_copy(qs.at[k], k, 3, 0, 1))
        send(*q_copy(qs.at[k], k, 1, 1, 3))

    def relay_queries(k):
        arrived = 3 if k % 2 == 0 else 1
        wait_queries(k, arrived)
        send(*q_copy(qp.at[pl.ds(k * 10 + place[arrived], 3)], k, 2, 2, 4 - arrived))

    def wait_queries(k, slot):
        args = q_copy(qs.at[k], k, slot, 0, 1)
        remote(*args).wait_recv()

    for i in (7, 8, 9):
        loads[i].wait()
    for r in range(3):
        rows = pl.ds(r * third, third)
        p = dot(xn[rows, :], wl[...])
        lq[rows, :] = (p[:, 0:256] * SCORE).astype(BF)
        lk[pl.ds(WINDOW + r * third, third), :] = p[:, 256:384].astype(BF)
        lv[pl.ds(WINDOW + r * third, third), :] = p[:, 384:512].astype(BF)

    def halo(ref, i, low):
        source, target, d = (ROWS, 0, 1) if low else (WINDOW, ROWS + WINDOW, NSP - 1)
        j = 2 * i + (0 if low else 1)
        return (
            ref.at[pl.ds(source, WINDOW)],
            ref.at[pl.ds(target, WINDOW)],
            h_s.at[j],
            h_r.at[j],
            sp_peer(d),
        )

    halos = [halo(ref, i, low) for i, ref in enumerate((lk, lv)) for low in (True, False)]
    for args in halos:
        send(*args)

    def attend(base, tiles, slots, count, tops=None, following=None):
        units = tiles * count // 2

        def where(u):
            halves = []
            for h in range(2):
                index = 2 * u + h
                halves.append((slots(index // tiles), base + lax.rem(index, tiles)))
            return halves

        def scores(halves, ref):
            tops = []
            for h, (t, g) in enumerate(halves):
                queries = jnp.concatenate([qp[2 * g], qp[2 * g + 1]], axis=1)
                s = dot(kall[t], queries)
                ref[h] = s
                tops.append(jnp.max(s, axis=0, keepdims=True))
            return tops

        def weigh(halves, ref, tops):
            for h, (t, g) in enumerate(halves):
                before = m[g]
                top = jnp.maximum(before, tops[h])
                factor = jnp.exp2(before - top)
                weights = jnp.exp2(ref[h] - top).astype(BF)
                result = dot(vall[t], weights)
                m[g] = top
                l[g] = l[g] * factor + result[HEAD : HEAD + 1]
                o[g] = o[g] * factor + result[:HEAD]

        if tops is None:
            tops = scores(where(0), s0)

        def body(i, tops):
            u = 2 * i
            later = scores(where(u + 1), s1)
            weigh(where(u), s0, tops)
            after = where(jnp.minimum(u + 2, units - 1))
            if following is not None:
                last = (i + 1) // (units // 2)
                after = [
                    (t * (1 - last) + ft * last, g * (1 - last) + fg * last)
                    for (t, g), (ft, fg) in zip(after, following)
                ]
            tops = scores(after, s0)
            weigh(where(u + 1), s1, later)
            return tops

        return lax.fori_loop(0, units // 2, body, tops)

    attend(EARLY // 2, 4, lambda i: i * 0, 1)

    wide = 3 * WINDOW
    row = lax.rem(lax.broadcasted_iota(jnp.int32, (2 * WINDOW, wide), 0), WINDOW)
    col = lax.broadcasted_iota(jnp.int32, (2 * WINDOW, wide), 1)
    near = (col >= row) & (col <= row + 2 * WINDOW)
    sink_rows = jnp.concatenate(
        [jnp.full((WINDOW, 1), sink[0] * LOG2E, F32), jnp.full((WINDOW, 1), sink[1] * LOG2E, F32)], axis=0
    )
    blocks = ROWS // WINDOW

    def banded(n, carry):
        at = pl.multiple_of(n * WINDOW, WINDOW)
        rows = lq[pl.ds(at, WINDOW), :]
        queries = jnp.concatenate([rows[:, :HEAD], rows[:, HEAD:]], axis=0)
        keys = lk[pl.ds(at, wide), :]
        s = lax.dot_general(queries, keys, (((1,), (1,)), ((), ())), preferred_element_type=F32)
        block = sp * blocks + n
        low = jnp.where(block == 0, WINDOW, 0)
        high = jnp.where(block == NSP * blocks - 1, 2 * WINDOW, wide)
        s = jnp.where(near & (col >= low) & (col < high), s, -1e30)
        top = jnp.maximum(jnp.max(s, axis=1, keepdims=True), sink_rows)
        lifted = jnp.exp2(s - top)
        total = jnp.sum(lifted, axis=1, keepdims=True) + jnp.exp2(sink_rows - top)
        result = dot(lifted.astype(BF), lv[pl.ds(at, wide), :]) / total
        lo[pl.ds(at, WINDOW), :] = jnp.concatenate([result[:WINDOW], result[WINDOW:]], axis=1).astype(BF)
        return carry

    lax.fori_loop(1, blocks - 1, banded, 0)

    remote(*k_up).wait_recv()
    send(*k_relay)
    remote(*v_down).wait_recv()
    send(*v_relay)
    for k in (0, 1):
        send_queries(k)
    remote(*k_down).wait_recv()
    remote(*v_up).wait_recv()
    attend(EARLY // 2, 4, lambda i: 1 + 2 * i, 2)
    relay_queries(0)
    for k in (2, 3):
        send_queries(k)
    for args in halos:
        remote(*args).wait_recv()
    lax.fori_loop(0, 2, lambda i, carry: banded(i * (blocks - 1), carry), 0)
    relay_queries(1)
    remote(*k_relay).wait_recv()
    remote(*v_relay).wait_recv()
    attend(EARLY // 2, 4, lambda i: i * 0 + 2, 1)

    def state(g):
        lanes = pl.ds(g % 2 * HEAD, HEAD)
        return m[g // 2, :, lanes], l[g // 2, :, lanes], o[g // 2, :, lanes]

    def packed(g):
        top, total, result = state(g)
        level = top + jnp.log2(total)
        high = level.astype(BF)
        rest = level - high.astype(F32)
        mid = rest.astype(BF)
        low = (rest - mid.astype(F32)).astype(BF)
        tail = jnp.concatenate([high, mid, low, jnp.zeros((13, HEAD), BF)], axis=0)
        return jnp.concatenate([(result * (1.0 / total)).astype(BF), tail], axis=0)

    def o_copy(k, s):
        return (osend.at[k, s], orecv.at[k, 4 - s], o_s.at[k, s], o_r.at[k, 4 - s], q_peer(s))

    def send_results(k, *targets):
        for s in targets:
            for i in range(3):
                osend[k, s, i] = packed(k * 10 + place[s] + i)
            send(*o_copy(k, s))

    def merge(k):
        for s in (1, 3, 2):
            remote(*o_copy(k, s)).wait_recv()
        merged = []
        for i in range(3):
            g = k * 10 + 9 if i == 2 else EARLY + 2 * k + i
            levels = []
            for s in (1, 2, 3):
                rows = orecv[k, s, i, pl.ds(HEAD, 16), :].astype(F32)
                levels.append(rows[0:1] + rows[1:2] + rows[2:3])
            highest, total, result = state(g)
            mine = highest + jnp.log2(total)
            top = functools.reduce(jnp.maximum, levels, mine)
            share = jnp.exp2(mine - top)
            shares = [jnp.exp2(level - top) for level in levels]
            whole = share + shares[0] + shares[1] + shares[2]
            acc = result * (share / (total * whole))
            for s in (1, 2, 3):
                acc += orecv[k, s, i, value_rows, :].astype(F32) * (shares[s - 1] / whole)
            merged.append(acc.T.astype(BF))
        one = jnp.concatenate([merged[0], merged[1][:64]], axis=0)
        two = jnp.concatenate([merged[1][64:], merged[2]], axis=0)
        features = jnp.concatenate([one, two, gather(lo, k)], axis=1)
        keep[k] = dot(features, wo[...])
        dsend[k] = keep[k, pl.ds(pl.multiple_of((1 - core) * 96, 16), 96), :].astype(BF)
        send(*d_copy(k))

    def d_copy(k):
        return (dsend.at[k], drecv.at[k], d_s.at[k], d_r.at[k], partner)

    half = D // 2

    def x_copy(i):
        if i < 2:
            return (x0.at[i], ra.at[i], x_s.at[i], x_r.at[i], x_peer(1 if i == 0 else 3))
        k, side = divmod(i - 2, 2)
        return (x12.at[k, side], r1.at[k, side], x_s.at[i], x_r.at[i], x_peer(1 if side == 0 else 3))

    def summed(k):
        remote(*d_copy(k)).wait_recv()
        return keep[k, pl.ds(pl.multiple_of(core * 96, 16), 96), :] + drecv[k].astype(F32)

    def scatter(k):
        total = summed(k)
        if k == 0:
            for i in range(2):
                x0[i] = total[:, i * half : i * half + half].astype(BF)
                send(*x_copy(i))
        elif k < 3:
            if k == 1:
                for i in range(2):
                    remote(*x_copy(i)).wait_recv()
            for side in range(2):
                mine = total[side * PART : side * PART + PART]
                passing = ra[side, pl.ds((k - 1) * PART, PART), :].astype(F32)
                if side == 0:
                    mine = jnp.concatenate([mine[:, :half] + passing, mine[:, half:]], axis=1)
                else:
                    mine = jnp.concatenate([mine[:, :half], mine[:, half:] + passing], axis=1)
                x12[k - 1, side] = mine.astype(BF)
                send(*x_copy(2 * k + side))
        else:
            for i in range(2, 6):
                remote(*x_copy(i)).wait_recv()
            for part in range(2):
                rows = slice(part * PART, part * PART + PART)
                both = r1[part, 0].astype(F32) + r1[part, 1].astype(F32)
                out[pl.ds(part * PART, PART), :] = (total[rows] + both).astype(BF)

    for i in (10, 11):
        loads[i].wait()
    def wait_block(k):
        wait_queries(k, 1 if k % 2 == 0 else 3)
        wait_queries(k, 2)

    wait_block(0)
    relay_queries(2)
    relay_queries(3)
    tops = None
    for k in range(BLOCKS):
        tops = attend(k * 5, 3, lambda i: i, SIDE, tops, [(0, k * 5 + 3), (0, k * 5 + 4)])
        send_results(k, 2, 1)
        if k > 1:
            scatter(k - 2)
        if k == BLOCKS - 1:
            merge(k - 1)
        following = None
        if k + 1 < BLOCKS:
            wait_block(k + 1)
            following = [(0, k * 5 + 5), (0, k * 5 + 6)]
        tops = attend(k * 5 + 3, 2, lambda i: i, SIDE, tops, following)
        send_results(k, 3)
        if k == BLOCKS - 1:
            scatter(k - 1)
        elif k > 0:
            merge(k - 1)
    merge(3)
    scatter(3)
    for copy in sends:
        copy.wait_send()


def shards(
    tokens,
    norm_gain,
    grid_query_weight,
    grid_key_weight,
    grid_value_weight,
    grid_query_gain,
    grid_key_gain,
    local_query_weight,
    local_key_weight,
    local_value_weight,
    sink_logit,
    grid_out_weight,
    local_out_weight,
):
    row_table, col_table = rope_tables()
    hbm = pl.BlockSpec(memory_space=pl.ANY)
    vmem = pl.BlockSpec(memory_space=pltpu.VMEM)
    smem = pl.BlockSpec(memory_space=pltpu.SMEM)
    dma = pltpu.SemaphoreType.DMA
    return pl.pallas_call(
        kernel,
        out_shape=jax.ShapeDtypeStruct((96, D), BF),
        in_specs=[hbm, vmem, hbm, hbm, hbm, vmem, vmem, hbm, hbm, hbm, smem, hbm, hbm, hbm, vmem],
        out_specs=vmem,
        scratch_shapes=[
            pltpu.VMEM((ROWS, D), BF),
            pltpu.VMEM((ROWS, D), BF),
            pltpu.VMEM((D, 256), BF),
            pltpu.VMEM((D, 256), BF),
            pltpu.VMEM((D, 512), BF),
            pltpu.VMEM((512, D), BF),
            pltpu.VMEM((2, 16, HEAD), F32),
            pltpu.VMEM((2, ROWS, HEAD), BF),
            pltpu.VMEM((BLOCKS, 3, HEAD, HEAD), BF),
            pltpu.VMEM((48, HEAD, HEAD), BF),
            pltpu.VMEM((SIDE, ROWS, HEAD), BF),
            pltpu.VMEM((SIDE, HEAD + 16, ROWS), BF),
            pltpu.VMEM((24, 1, 2 * HEAD), F32),
            pltpu.VMEM((24, 1, 2 * HEAD), F32),
            pltpu.VMEM((24, HEAD, 2 * HEAD), F32),
            pltpu.VMEM((2, ROWS, 256), F32),
            pltpu.VMEM((2, ROWS, 256), F32),
            pltpu.VMEM((ROWS, 256), BF),
            pltpu.VMEM((ROWS + 2 * WINDOW, HEAD), BF),
            pltpu.VMEM((ROWS + 2 * WINDOW, HEAD), BF),
            pltpu.VMEM((ROWS, 256), BF),
            pltpu.VMEM((BLOCKS, 4, 3, HEAD + 16, HEAD), BF),
            pltpu.VMEM((BLOCKS, 4, 3, HEAD + 16, HEAD), BF),
            pltpu.VMEM((BLOCKS, 192, D), F32),
            pltpu.VMEM((BLOCKS, 96, D), BF),
            pltpu.VMEM((BLOCKS, 96, D), BF),
            pltpu.VMEM((2, 96, D // 2), BF),
            pltpu.VMEM((2, 2, PART, D), BF),
            pltpu.VMEM((2, 96, D // 2), BF),
            pltpu.VMEM((2, 2, PART, D), BF),
            dma((12,)),
            dma((6,)),
            dma((2, 4)),
            dma((BLOCKS, 3)),
            dma((BLOCKS, 4)),
            dma((4,)),
            dma((4,)),
            dma((BLOCKS, 4)),
            dma((BLOCKS, 4)),
            dma((BLOCKS,)),
            dma((BLOCKS,)),
            dma((6,)),
            dma((6,)),
        ],
        compiler_params=pltpu.CompilerParams(
            collective_id=0, has_side_effects=True, vmem_limit_bytes=60 * 2**20
        ),
    )(
        tokens,
        norm_gain.reshape(1, D),
        grid_query_weight,
        grid_key_weight,
        grid_value_weight,
        grid_query_gain.reshape(1, HEAD),
        grid_key_gain.reshape(1, HEAD),
        local_query_weight,
        local_key_weight,
        local_value_weight,
        sink_logit,
        grid_out_weight,
        local_out_weight,
        jnp.asarray(row_table),
        jnp.asarray(col_table),
    )


def solution(mesh):
    in_specs = (
        P("sp", None),
        P(),
        P(None, "tp"),
        P(None, "tp"),
        P(None, "tp"),
        P(),
        P(),
        P(None, "tp"),
        P(None, "tp"),
        P(None, "tp"),
        P("tp"),
        P("tp", None),
        P("tp", None),
    )
    out_specs = P(("sp", "tp"), None)
    return jax.shard_map(shards, mesh=mesh, in_specs=in_specs, out_specs=out_specs, check_vma=False)
```

```python
import functools
import math

import jax
import jax.numpy as jnp
import numpy as np
from jax import lax
from jax.experimental import pallas as pl
from jax.experimental.pallas import tpu as pltpu
from jax.sharding import PartitionSpec as P

D = 2048
HEAD = 128
WINDOW = 128
GRID_W = 64
ROWS = 768
EPSILON = 1e-06
ROPE_BASE = 10000.0
LOG2E = math.log2(math.e)
SCORE = HEAD ** (-0.5) * LOG2E
NSP = 16
SIDE = 4
BLOCKS = 4
CHUNK = 32
PART = 48
EARLY = 40
BF = jnp.bfloat16
F32 = jnp.float32
MESH = pl.DeviceIdType.MESH


def dot(a, b):
    return jnp.dot(a, b, preferred_element_type=F32)


def rope_tables():
    half = HEAD // 2
    inverse = ROPE_BASE ** (-np.arange(0, half, 2, dtype=np.float64) / half)
    sign = np.concatenate([-np.ones(half // 2), np.ones(half // 2)])

    def table(count):
        angle = np.arange(count)[:, None] * np.concatenate([inverse, inverse])
        return np.cos(angle), np.sin(angle) * sign

    rows = np.zeros((2, NSP, 16, HEAD), np.float32)
    cosine, sine = table(NSP * ROWS // GRID_W)
    per = ROWS // GRID_W
    rows[0, :, :per, :half] = cosine.reshape(NSP, per, half)
    rows[1, :, :per, :half] = sine.reshape(NSP, per, half)
    cols = np.zeros((2, GRID_W, HEAD), np.float32)
    cosine, sine = table(GRID_W)
    cols[0, :, half:] = cosine
    cols[1, :, half:] = sine
    return np.ascontiguousarray(rows.transpose(1, 0, 2, 3)), cols


def kernel(
    tokens,
    gain,
    wq,
    wk,
    wv,
    gain_q,
    gain_k,
    lwq,
    lwk,
    lwv,
    sink,
    wog,
    wol,
    row_table,
    col_table,
    out,
    xs,
    xn,
    wkv,
    wqg,
    wl,
    wo,
    rows_tab,
    qr,
    qs,
    qp,
    kall,
    vall,
    m,
    l,
    o,
    s0,
    s1,
    lq,
    lk,
    lv,
    lo,
    osend,
    orecv,
    keep,
    dsend,
    drecv,
    x0,
    x12,
    ra,
    r1,
    in_sem,
    kv_s,
    kv_r,
    q_s,
    q_r,
    h_s,
    h_r,
    o_s,
    o_r,
    d_s,
    d_r,
    x_s,
    x_r,
):
    sp = lax.axis_index("sp")
    tp = lax.axis_index("tp")
    core = lax.rem(tp, 2)
    x = tp // 2
    z = sp // SIDE
    y = lax.rem(sp, SIDE)

    def along_z(d):
        return lax.rem(z + d, SIDE) * SIDE + y

    def along_y(d):
        return z * SIDE + lax.rem(y + d, SIDE)

    def q_peer(d):
        return {"sp": along_z(d) * (1 - core) + along_y(d) * core, "tp": tp}

    def kv_peer(d):
        return {"sp": along_z(d) * core + along_y(d) * (1 - core), "tp": tp}

    def sp_peer(d):
        return {"sp": lax.rem(sp + d, NSP), "tp": tp}

    def x_peer(d):
        return {"sp": sp, "tp": lax.rem(x + d, SIDE) * 2 + core}

    partner = {"sp": sp, "tp": x * 2 + 1 - core}

    def remote(src, dst, send, recv, peer):
        return pltpu.make_async_remote_copy(
            src_ref=src, dst_ref=dst, send_sem=send, recv_sem=recv, device_id=peer, device_id_type=MESH
        )

    def local(src, dst, i):
        return pltpu.make_async_copy(src, dst, in_sem.at[i])

    third = ROWS // 3
    loads = [
        local(tokens.at[pl.ds(0, third)], xs.at[pl.ds(0, third)], 0),
        local(wk, wkv.at[:, pl.ds(0, 128)], 1),
        local(wv, wkv.at[:, pl.ds(128, 128)], 2),
        local(row_table.at[sp], rows_tab, 4),
        local(tokens.at[pl.ds(third, third)], xs.at[pl.ds(third, third)], 5),
        local(tokens.at[pl.ds(2 * third, third)], xs.at[pl.ds(2 * third, third)], 6),
        local(wq, wqg, 3),
        local(lwq, wl.at[:, pl.ds(0, 256)], 7),
        local(lwk, wl.at[:, pl.ds(256, 128)], 8),
        local(lwv, wl.at[:, pl.ds(384, 128)], 9),
        local(wog, wo.at[pl.ds(0, 256)], 10),
        local(wol, wo.at[pl.ds(256, 256)], 11),
    ]
    loads = dict(zip((0, 1, 2, 4, 5, 6, 3, 7, 8, 9, 10, 11), loads))
    for i in (0, 1, 2, 4, 5, 6):
        loads[i].start()

    barrier = pltpu.get_barrier_semaphore()
    peers = [q_peer(1), q_peer(2), q_peer(3), kv_peer(1), kv_peer(3), sp_peer(1), sp_peer(NSP - 1)]
    peers += [x_peer(1), x_peer(3), partner]
    for peer in peers:
        pl.semaphore_signal(barrier, inc=1, device_id=peer, device_id_type=MESH)

    m[...] = jnp.full_like(m, -1e30)
    l[...] = jnp.zeros_like(l)
    o[...] = jnp.zeros_like(o)
    vall[:, pl.ds(HEAD, 16), :] = jnp.ones((SIDE, 16, ROWS), BF)

    lane = lax.broadcasted_iota(jnp.int32, (third, HEAD), 1)
    first_half = lax.rem(lane, 64) < 32

    def norm(r):
        for c in range(third // CHUNK):
            rows = pl.ds(r * third + c * CHUNK, CHUNK)
            squares = jnp.zeros((CHUNK, HEAD), F32)
            for j in range(D // HEAD):
                part = xs[rows, pl.ds(j * HEAD, HEAD)].astype(F32)
                squares += part * part
            factor = lax.rsqrt(jnp.sum(squares, axis=-1, keepdims=True) / D + EPSILON)
            for j in range(D // HEAD):
                cols = pl.ds(j * HEAD, HEAD)
                xn[rows, cols] = (xs[rows, cols].astype(F32) * factor * gain[:, cols]).astype(BF)

    def rope(u, gain_row, r):
        mean = jnp.mean(u * u, axis=-1, keepdims=True)
        u = u * lax.rsqrt(mean + EPSILON) * gain_row
        swapped = jnp.where(first_half, pltpu.roll(u, HEAD - 32, 1), pltpu.roll(u, 32, 1))
        per = third // GRID_W

        def table(which):
            return jnp.concatenate(
                [col_table[which] + rows_tab[which, pl.ds(r * per + i, 1), :] for i in range(per)], axis=0
            )

        return (u * table(0) + swapped * table(1)).astype(BF)

    def project_keys(r):
        rows = pl.ds(r * third, third)
        p = dot(xn[rows, :], wkv[...])
        kall[0, rows, :] = rope(p[:, 0:128], gain_k[...], r)
        vall[0, pl.ds(0, HEAD), rows] = p[:, 128:256].T.astype(BF)

    def project_queries(r):
        rows = pl.ds(r * third, third)
        p = dot(xn[rows, :], wqg[...])
        scaled = gain_q[...] * SCORE
        qr[0, rows, :] = rope(p[:, 0:128], scaled, r)
        qr[1, rows, :] = rope(p[:, 128:256], scaled, r)

    loads[0].wait()
    loads[3].start()
    norm(0)
    for i in (1, 2, 4, 5):
        loads[i].wait()
    for i in (7, 8, 9, 10, 11):
        loads[i].start()
    norm(1)
    project_keys(0)
    loads[6].wait()
    norm(2)
    project_keys(1)
    project_keys(2)

    pl.semaphore_wait(barrier, len(peers))
    value_rows = pl.ds(0, HEAD)
    sends = []

    def send(*args):
        copy = remote(*args)
        copy.start()
        sends.append(copy)

    def k_copy(slot_from, slot_to, s, d):
        return (kall.at[slot_from], kall.at[slot_to], kv_s.at[s], kv_r.at[0, slot_to], kv_peer(d))

    def v_copy(slot_from, slot_to, s, d):
        return (
            vall.at[slot_from, value_rows],
            vall.at[slot_to, value_rows],
            kv_s.at[s],
            kv_r.at[1, slot_to],
            kv_peer(d),
        )

    k_up, k_down = k_copy(0, 3, 0, 1), k_copy(0, 1, 1, 3)
    v_up, v_down = v_copy(0, 3, 2, 1), v_copy(0, 1, 3, 3)
    for args in (k_up, v_down, k_down, v_up):
        send(*args)
    k_relay, v_relay = k_copy(3, 2, 4, 1), v_copy(1, 2, 5, 3)

    loads[3].wait()
    for r in range(3):
        project_queries(r)
    ahead, behind, across = (lax.rem(x + d, SIDE) * 192 for d in (1, 3, 2))
    own = x * 192
    starts = (
        (across, across + 48, across + 96, across + 144),
        (ahead, behind, ahead + 96, behind + 96),
        (ahead + 48, behind + 48, ahead + 144, behind + 144),
        (own, own + 48, own + 96, own + 144),
    )

    def gather(ref, k):
        return jnp.concatenate([ref[pl.ds(pl.multiple_of(s, 16), PART), :] for s in starts[k]], axis=0)

    for k in range(BLOCKS):
        one, two = gather(qr.at[0], k), gather(qr.at[1], k)
        pieces = (one[:128], jnp.concatenate([one[128:], two[:64]], axis=0), two[64:])
        for i, piece in enumerate(pieces):
            turned = piece.astype(F32).T.astype(BF)
            qs[k, i] = turned
            qp[k * 10 + 9 if i == 2 else EARLY + 2 * k + i] = turned

    place = {2: 0, 1: 3, 3: 6}

    def q_copy(source, k, slot, s, d):
        return (source, qp.at[pl.ds(k * 10 + place[slot], 3)], q_s.at[k, s], q_r.at[k, slot], q_peer(d))

    def send_queries(k):
        send(*q_copy(qs.at[k], k, 3, 0, 1))
        send(*q_copy(qs.at[k], k, 1, 1, 3))

    def relay_queries(k):
        arrived = 3 if k % 2 == 0 else 1
        wait_queries(k, arrived)
        send(*q_copy(qp.at[pl.ds(k * 10 + place[arrived], 3)], k, 2, 2, 4 - arrived))

    def wait_queries(k, slot):
        args = q_copy(qs.at[k], k, slot, 0, 1)
        remote(*args).wait_recv()

    send_queries(0)

    for i in (7, 8, 9):
        loads[i].wait()
    for r in range(3):
        rows = pl.ds(r * third, third)
        p = dot(xn[rows, :], wl[...])
        lq[rows, :] = (p[:, 0:256] * SCORE).astype(BF)
        lk[pl.ds(WINDOW + r * third, third), :] = p[:, 256:384].astype(BF)
        lv[pl.ds(WINDOW + r * third, third), :] = p[:, 384:512].astype(BF)

    def halo(ref, i, low):
        source, target, d = (ROWS, 0, 1) if low else (WINDOW, ROWS + WINDOW, NSP - 1)
        j = 2 * i + (0 if low else 1)
        return (
            ref.at[pl.ds(source, WINDOW)],
            ref.at[pl.ds(target, WINDOW)],
            h_s.at[j],
            h_r.at[j],
            sp_peer(d),
        )

    halos = [halo(ref, i, low) for i, ref in enumerate((lk, lv)) for low in (True, False)]
    for args in halos:
        send(*args)

    def attend(base, tiles, slots, count, tops=None, following=None):
        units = tiles * count // 2

        def where(u):
            halves = []
            for h in range(2):
                index = 2 * u + h
                halves.append((slots(index // tiles), base + lax.rem(index, tiles)))
            return halves

        def scores(halves, ref):
            tops = []
            for h, (t, g) in enumerate(halves):
                queries = jnp.concatenate([qp[2 * g], qp[2 * g + 1]], axis=1)
                s = dot(kall[t], queries)
                ref[h] = s
                tops.append(jnp.max(s, axis=0, keepdims=True))
            return tops

        def weigh(halves, ref, tops):
            for h, (t, g) in enumerate(halves):
                before = m[g]
                top = jnp.maximum(before, tops[h])
                factor = jnp.exp2(before - top)
                weights = jnp.exp2(ref[h] - top).astype(BF)
                result = dot(vall[t], weights)
                m[g] = top
                l[g] = l[g] * factor + result[HEAD : HEAD + 1]
                o[g] = o[g] * factor + result[:HEAD]

        if tops is None:
            tops = scores(where(0), s0)

        def body(i, tops):
            u = 2 * i
            later = scores(where(u + 1), s1)
            weigh(where(u), s0, tops)
            after = where(jnp.minimum(u + 2, units - 1))
            if following is not None:
                last = (i + 1) // (units // 2)
                after = [
                    (t * (1 - last) + ft * last, g * (1 - last) + fg * last)
                    for (t, g), (ft, fg) in zip(after, following)
                ]
            tops = scores(after, s0)
            weigh(where(u + 1), s1, later)
            return tops

        return lax.fori_loop(0, units // 2, body, tops)

    attend(EARLY // 2, 4, lambda i: i * 0, 1)

    wide = 3 * WINDOW
    row = lax.rem(lax.broadcasted_iota(jnp.int32, (2 * WINDOW, wide), 0), WINDOW)
    col = lax.broadcasted_iota(jnp.int32, (2 * WINDOW, wide), 1)
    near = (col >= row) & (col <= row + 2 * WINDOW)
    sink_rows = jnp.concatenate(
        [jnp.full((WINDOW, 1), sink[0] * LOG2E, F32), jnp.full((WINDOW, 1), sink[1] * LOG2E, F32)], axis=0
    )
    blocks = ROWS // WINDOW

    def banded(n, carry):
        at = pl.multiple_of(n * WINDOW, WINDOW)
        rows = lq[pl.ds(at, WINDOW), :]
        queries = jnp.concatenate([rows[:, :HEAD], rows[:, HEAD:]], axis=0)
        keys = lk[pl.ds(at, wide), :]
        s = lax.dot_general(queries, keys, (((1,), (1,)), ((), ())), preferred_element_type=F32)
        block = sp * blocks + n
        low = jnp.where(block == 0, WINDOW, 0)
        high = jnp.where(block == NSP * blocks - 1, 2 * WINDOW, wide)
        s = jnp.where(near & (col >= low) & (col < high), s, -1e30)
        top = jnp.maximum(jnp.max(s, axis=1, keepdims=True), sink_rows)
        lifted = jnp.exp2(s - top)
        total = jnp.sum(lifted, axis=1, keepdims=True) + jnp.exp2(sink_rows - top)
        result = dot(lifted.astype(BF), lv[pl.ds(at, wide), :]) / total
        lo[pl.ds(at, WINDOW), :] = jnp.concatenate([result[:WINDOW], result[WINDOW:]], axis=1).astype(BF)
        return carry

    lax.fori_loop(1, blocks - 1, banded, 0)

    remote(*k_up).wait_recv()
    send(*k_relay)
    remote(*v_down).wait_recv()
    send(*v_relay)
    relay_queries(0)
    send_queries(1)
    remote(*k_down).wait_recv()
    remote(*v_up).wait_recv()
    attend(EARLY // 2, 4, lambda i: 1 + 2 * i, 2)
    for k in (2, 3):
        send_queries(k)
    for args in halos:
        remote(*args).wait_recv()
    lax.fori_loop(0, 2, lambda i, carry: banded(i * (blocks - 1), carry), 0)
    relay_queries(1)
    remote(*k_relay).wait_recv()
    remote(*v_relay).wait_recv()
    attend(EARLY // 2, 4, lambda i: i * 0 + 2, 1)

    def state(g):
        lanes = pl.ds(g % 2 * HEAD, HEAD)
        return m[g // 2, :, lanes], l[g // 2, :, lanes], o[g // 2, :, lanes]

    def packed(g):
        top, total, result = state(g)
        level = top + jnp.log2(total)
        high = level.astype(BF)
        rest = level - high.astype(F32)
        mid = rest.astype(BF)
        low = (rest - mid.astype(F32)).astype(BF)
        tail = jnp.concatenate([high, mid, low, jnp.zeros((13, HEAD), BF)], axis=0)
        return jnp.concatenate([(result * (1.0 / total)).astype(BF), tail], axis=0)

    def o_copy(k, s):
        return (osend.at[k, s], orecv.at[k, 4 - s], o_s.at[k, s], o_r.at[k, 4 - s], q_peer(s))

    def send_results(k, *targets):
        for s in targets:
            for i in range(3):
                osend[k, s, i] = packed(k * 10 + place[s] + i)
            send(*o_copy(k, s))

    def merge(k):
        for s in (1, 3, 2):
            remote(*o_copy(k, s)).wait_recv()
        merged = []
        for i in range(3):
            g = k * 10 + 9 if i == 2 else EARLY + 2 * k + i
            levels = []
            for s in (1, 2, 3):
                rows = orecv[k, s, i, pl.ds(HEAD, 16), :].astype(F32)
                levels.append(rows[0:1] + rows[1:2] + rows[2:3])
            highest, total, result = state(g)
            mine = highest + jnp.log2(total)
            top = functools.reduce(jnp.maximum, levels, mine)
            share = jnp.exp2(mine - top)
            shares = [jnp.exp2(level - top) for level in levels]
            whole = share + shares[0] + shares[1] + shares[2]
            acc = result * (share / (total * whole))
            for s in (1, 2, 3):
                acc += orecv[k, s, i, value_rows, :].astype(F32) * (shares[s - 1] / whole)
            merged.append(acc.T.astype(BF))
        one = jnp.concatenate([merged[0], merged[1][:64]], axis=0)
        two = jnp.concatenate([merged[1][64:], merged[2]], axis=0)
        features = jnp.concatenate([one, two, gather(lo, k)], axis=1)
        keep[k] = dot(features, wo[...])
        dsend[k] = keep[k, pl.ds(pl.multiple_of((1 - core) * 96, 16), 96), :].astype(BF)
        send(*d_copy(k))

    def d_copy(k):
        return (dsend.at[k], drecv.at[k], d_s.at[k], d_r.at[k], partner)

    half = D // 2

    def x_copy(i):
        if i < 2:
            return (x0.at[i], ra.at[i], x_s.at[i], x_r.at[i], x_peer(1 if i == 0 else 3))
        k, side = divmod(i - 2, 2)
        return (x12.at[k, side], r1.at[k, side], x_s.at[i], x_r.at[i], x_peer(1 if side == 0 else 3))

    def summed(k):
        remote(*d_copy(k)).wait_recv()
        return keep[k, pl.ds(pl.multiple_of(core * 96, 16), 96), :] + drecv[k].astype(F32)

    def scatter(k):
        total = summed(k)
        if k == 0:
            for i in range(2):
                x0[i] = total[:, i * half : i * half + half].astype(BF)
                send(*x_copy(i))
        elif k < 3:
            if k == 1:
                for i in range(2):
                    remote(*x_copy(i)).wait_recv()
            for side in range(2):
                mine = total[side * PART : side * PART + PART]
                passing = ra[side, pl.ds((k - 1) * PART, PART), :].astype(F32)
                if side == 0:
                    mine = jnp.concatenate([mine[:, :half] + passing, mine[:, half:]], axis=1)
                else:
                    mine = jnp.concatenate([mine[:, :half], mine[:, half:] + passing], axis=1)
                x12[k - 1, side] = mine.astype(BF)
                send(*x_copy(2 * k + side))
        else:
            for i in range(2, 6):
                remote(*x_copy(i)).wait_recv()
            for part in range(2):
                rows = slice(part * PART, part * PART + PART)
                both = r1[part, 0].astype(F32) + r1[part, 1].astype(F32)
                out[pl.ds(part * PART, PART), :] = (total[rows] + both).astype(BF)

    for i in (10, 11):
        loads[i].wait()
    def wait_block(k):
        wait_queries(k, 1 if k % 2 == 0 else 3)
        wait_queries(k, 2)

    wait_block(0)
    relay_queries(2)
    relay_queries(3)
    tops = None
    for k in range(BLOCKS):
        tops = attend(k * 5, 3, lambda i: i, SIDE, tops, [(0, k * 5 + 3), (0, k * 5 + 4)])
        send_results(k, 2, 1)
        if k > 1:
            scatter(k - 2)
        if k == BLOCKS - 1:
            merge(k - 1)
        following = None
        if k + 1 < BLOCKS:
            wait_block(k + 1)
            following = [(0, k * 5 + 5), (0, k * 5 + 6)]
        tops = attend(k * 5 + 3, 2, lambda i: i, SIDE, tops, following)
        send_results(k, 3)
        if k == BLOCKS - 1:
            scatter(k - 1)
        elif k > 0:
            merge(k - 1)
    merge(3)
    scatter(3)
    for copy in sends:
        copy.wait_send()


def shards(
    tokens,
    norm_gain,
    grid_query_weight,
    grid_key_weight,
    grid_value_weight,
    grid_query_gain,
    grid_key_gain,
    local_query_weight,
    local_key_weight,
    local_value_weight,
    sink_logit,
    grid_out_weight,
    local_out_weight,
):
    row_table, col_table = rope_tables()
    hbm = pl.BlockSpec(memory_space=pl.ANY)
    vmem = pl.BlockSpec(memory_space=pltpu.VMEM)
    smem = pl.BlockSpec(memory_space=pltpu.SMEM)
    dma = pltpu.SemaphoreType.DMA
    return pl.pallas_call(
        kernel,
        out_shape=jax.ShapeDtypeStruct((96, D), BF),
        in_specs=[hbm, vmem, hbm, hbm, hbm, vmem, vmem, hbm, hbm, hbm, smem, hbm, hbm, hbm, vmem],
        out_specs=vmem,
        scratch_shapes=[
            pltpu.VMEM((ROWS, D), BF),
            pltpu.VMEM((ROWS, D), BF),
            pltpu.VMEM((D, 256), BF),
            pltpu.VMEM((D, 256), BF),
            pltpu.VMEM((D, 512), BF),
            pltpu.VMEM((512, D), BF),
            pltpu.VMEM((2, 16, HEAD), F32),
            pltpu.VMEM((2, ROWS, HEAD), BF),
            pltpu.VMEM((BLOCKS, 3, HEAD, HEAD), BF),
            pltpu.VMEM((48, HEAD, HEAD), BF),
            pltpu.VMEM((SIDE, ROWS, HEAD), BF),
            pltpu.VMEM((SIDE, HEAD + 16, ROWS), BF),
            pltpu.VMEM((24, 1, 2 * HEAD), F32),
            pltpu.VMEM((24, 1, 2 * HEAD), F32),
            pltpu.VMEM((24, HEAD, 2 * HEAD), F32),
            pltpu.VMEM((2, ROWS, 256), F32),
            pltpu.VMEM((2, ROWS, 256), F32),
            pltpu.VMEM((ROWS, 256), BF),
            pltpu.VMEM((ROWS + 2 * WINDOW, HEAD), BF),
            pltpu.VMEM((ROWS + 2 * WINDOW, HEAD), BF),
            pltpu.VMEM((ROWS, 256), BF),
            pltpu.VMEM((BLOCKS, 4, 3, HEAD + 16, HEAD), BF),
            pltpu.VMEM((BLOCKS, 4, 3, HEAD + 16, HEAD), BF),
            pltpu.VMEM((BLOCKS, 192, D), F32),
            pltpu.VMEM((BLOCKS, 96, D), BF),
            pltpu.VMEM((BLOCKS, 96, D), BF),
            pltpu.VMEM((2, 96, D // 2), BF),
            pltpu.VMEM((2, 2, PART, D), BF),
            pltpu.VMEM((2, 96, D // 2), BF),
            pltpu.VMEM((2, 2, PART, D), BF),
            dma((12,)),
            dma((6,)),
            dma((2, 4)),
            dma((BLOCKS, 3)),
            dma((BLOCKS, 4)),
            dma((4,)),
            dma((4,)),
            dma((BLOCKS, 4)),
            dma((BLOCKS, 4)),
            dma((BLOCKS,)),
            dma((BLOCKS,)),
            dma((6,)),
            dma((6,)),
        ],
        compiler_params=pltpu.CompilerParams(
            collective_id=0, has_side_effects=True, vmem_limit_bytes=60 * 2**20
        ),
    )(
        tokens,
        norm_gain.reshape(1, D),
        grid_query_weight,
        grid_key_weight,
        grid_value_weight,
        grid_query_gain.reshape(1, HEAD),
        grid_key_gain.reshape(1, HEAD),
        local_query_weight,
        local_key_weight,
        local_value_weight,
        sink_logit,
        grid_out_weight,
        local_out_weight,
        jnp.asarray(row_table),
        jnp.asarray(col_table),
    )


def solution(mesh):
    in_specs = (
        P("sp", None),
        P(),
        P(None, "tp"),
        P(None, "tp"),
        P(None, "tp"),
        P(),
        P(),
        P(None, "tp"),
        P(None, "tp"),
        P(None, "tp"),
        P("tp"),
        P("tp", None),
        P("tp", None),
    )
    out_specs = P(("sp", "tp"), None)
    return jax.shard_map(shards, mesh=mesh, in_specs=in_specs, out_specs=out_specs, check_vma=False)
```
